32 devices in a mesh: gr: 2 (over x), fs: 4 (over z), tp: 4 (over y, core).
Axes of the slice: x: 2, y: 2, z: 4, core: 2. Of those that a mesh axis runs over, the one named last changes fastest.
Arguments:
- prompt: bfloat16 [4096, 2048], P(('gr', 'fs')), may hold values from -6 to 6
- gain_first: float32 [2048], P(('gr', 'fs')), may hold values from 0.1 to 1.9
- gate_first: float32 [2048, 2816], P(('gr', 'fs'), 'tp'), may hold values from -0.125 to 0.125
- up_first: float32 [2048, 2816], P(('gr', 'fs'), 'tp'), may hold values from -0.125 to 0.125
- down_first: float32 [2816, 2048], P(('gr', 'fs'), 'tp'), may hold values from -0.109375 to 0.109375
- gain_second: float32 [2048], P(('gr', 'fs')), may hold values from 0.1 to 1.9
- gate_second: float32 [2048, 2816], P(('gr', 'fs'), 'tp'), may hold values from -0.125 to 0.125
- up_second: float32 [2048, 2816], P(('gr', 'fs'), 'tp'), may hold values from -0.125 to 0.125
- down_second: float32 [2816, 2048], P(('gr', 'fs'), 'tp'), may hold values from -0.109375 to 0.109375
Outputs:
- serve_gate_first: bfloat16 [2048, 2816], P(None, 'tp')
- serve_up_first: bfloat16 [2048, 2816], P(None, 'tp')
- serve_down_first: bfloat16 [2816, 2048], P('tp')
- serve_gate_second: bfloat16 [2048, 2816], P(None, 'tp')
- serve_up_second: bfloat16 [2048, 2816], P(None, 'tp')
- serve_down_second: bfloat16 [2816, 2048], P('tp')
- mixed: bfloat16 [4096, 2048], P(('gr', 'fs', 'tp'))
The draws below stay inside these ranges and needn't reach their ends.
All inputs are finite; a program needn't handle non-finite values.
Results may differ from the reference program's by a relative error of at most 0.0085.
Values may be sent and summed in bfloat16 or wider, within the bound.
A program may use at most 128 MiB of HBM per device.

```python
import jax
import jax.numpy as jnp
from jax import lax

D = 2048
FF = 2816
TOKENS = 4096
N_TP = 4


def shard_levels(stream_key, dims, pieces, low, high):
    def one(dim, shards_of):
        steps = jax.random.uniform(jax.random.fold_in(jax.random.fold_in(stream_key, 6), dim), (shards_of,), jnp.float32, low / len(pieces), high / len(pieces))
        return jnp.repeat(jnp.exp(steps), dims[dim] // shards_of).reshape((-1,) + (1,) * (len(dims) - dim - 1))

    level = one(*pieces[0])
    for cut in pieces[1:]:
        level = level * one(*cut)
    return level


def normal_values(stream_key, shape, scale, most, pieces=(), dtype=jnp.bfloat16):
    gain = shard_levels(stream_key, shape, pieces, -0.22, 0.18) if pieces else 1.0
    result = jax.random.normal(stream_key, shape, jnp.float32) * scale * gain
    return jnp.minimum(jnp.maximum(result, -most), most).astype(dtype)


def setup_inputs(seed: int = 0) -> dict:
    keys = jax.random.split(jax.random.key(seed), 10)
    prompt = normal_values(keys[0], (TOKENS, D), 1.0, 6.0, ((0, 8),))
    gain_first = jnp.clip(1.0 + 0.18 * jax.random.normal(keys[1], (D,), jnp.float32), 0.1, 1.9)
    gate_first = normal_values(keys[2], (D, FF), D ** -0.5, 0.125, ((0, 8), (1, 4)), jnp.float32)
    up_first = normal_values(keys[3], (D, FF), D ** -0.5, 0.125, ((0, 8), (1, 4)), jnp.float32)
    down_first = normal_values(keys[4], (FF, D), FF ** -0.5, 0.109375, ((0, 8), (1, 4)), jnp.float32)
    gain_second = jnp.clip(1.0 + 0.18 * jax.random.normal(keys[5], (D,), jnp.float32), 0.1, 1.9)
    gate_second = normal_values(keys[6], (D, FF), D ** -0.5, 0.125, ((0, 8), (1, 4)), jnp.float32)
    up_second = normal_values(keys[7], (D, FF), D ** -0.5, 0.125, ((0, 8), (1, 4)), jnp.float32)
    down_second = normal_values(keys[8], (FF, D), FF ** -0.5, 0.109375, ((0, 8), (1, 4)), jnp.float32)
    return dict(prompt=prompt, gain_first=gain_first, gate_first=gate_first, up_first=up_first, down_first=down_first, gain_second=gain_second, gate_second=gate_second, up_second=up_second, down_second=down_second)


def normalize(rows):
    rows = rows.astype(jnp.float32)
    scale = jax.lax.rsqrt(lax.optimization_barrier(jnp.mean(rows * rows, axis=-1, keepdims=True)) + 1e-06)
    return (rows * scale).astype(jnp.bfloat16)

def layer_branch(normed, w_gate, w_up, w_down):
    gate = jnp.dot(normed, w_gate, preferred_element_type=jnp.float32)
    upper = jnp.dot(normed, w_up, preferred_element_type=jnp.float32)
    hidden = (jax.nn.silu(gate) * upper).astype(jnp.bfloat16)
    width = hidden.shape[1] // N_TP
    total = jnp.zeros((hidden.shape[0], w_down.shape[1]), jnp.float32)
    for block in range(N_TP):
        part = jnp.dot(hidden[:, block * width:(block + 1) * width], w_down[block * width:(block + 1) * width, :], preferred_element_type=jnp.float32)
        total = total + part.astype(jnp.bfloat16).astype(jnp.float32)
    return total

def reference(prompt, gain_first, gate_first, up_first, down_first, gain_second, gate_second, up_second, down_second):
    serve_gate_first = (gain_first[:, None] * gate_first).astype(jnp.bfloat16)
    serve_up_first = (gain_first[:, None] * up_first).astype(jnp.bfloat16)
    serve_down_first = down_first.astype(jnp.bfloat16)
    serve_gate_second = (gain_second[:, None] * gate_second).astype(jnp.bfloat16)
    serve_up_second = (gain_second[:, None] * up_second).astype(jnp.bfloat16)
    serve_down_second = down_second.astype(jnp.bfloat16)
    stream = prompt.astype(jnp.float32) + 0.5 * layer_branch(normalize(prompt), serve_gate_first, serve_up_first, serve_down_first)
    mixed = (stream + 0.5 * layer_branch(normalize(stream), serve_gate_second, serve_up_second, serve_down_second)).astype(jnp.bfloat16)
    return (serve_gate_first, serve_up_first, serve_down_first, serve_gate_second, serve_up_second, serve_down_second, mixed)
```

```python
import functools

import jax
import jax.numpy as jnp
from jax import lax
from jax.experimental import pallas as pl
from jax.experimental.pallas import tpu as pltpu
from jax.sharding import PartitionSpec as P

MESH = pl.DeviceIdType.MESH


def gather_kernel(
    n_gr,
    n_fs,
    n_tp,
    gain_ref,
    gate_ref,
    up_ref,
    down_ref,
    gate_out,
    up_out,
    down_out,
    down_own,
    line_send,
    line_recv,
    pair_send,
    pair_recv,
    part_send,
    part_recv,
):
    g, f, t = lax.axis_index("gr"), lax.axis_index("fs"), lax.axis_index("tp")
    per = n_gr * n_fs // n_tp
    cols = down_ref.shape[1]
    first = lax.rem(t * per, n_fs)
    home = (t * per) // n_fs
    row = g * n_fs + f
    owner = row // per
    slot = lax.rem(row, per)

    width = gate_ref.shape[1]

    def place(ref, origin):
        if len(ref.shape) == 3:
            return ref.at[origin]
        return ref.at[:, pl.ds(pl.multiple_of(origin * width, 128), width)]

    gain = gain_ref[...]
    place(gate_out, row)[...] = (gain * gate_ref[...]).astype(jnp.bfloat16)
    place(up_out, row)[...] = (gain * up_ref[...]).astype(jnp.bfloat16)
    down_own[...] = down_ref[...].astype(jnp.bfloat16)

    @pl.when(owner == t)
    def _():
        down_out[slot, :, pl.ds(pl.multiple_of(t * cols, 128), cols)] = down_ref[...].astype(
            jnp.bfloat16
        )

    barrier = pltpu.get_barrier_semaphore()
    for dg in range(n_gr):
        for dt in range(n_tp):
            if dg or dt:
                pl.semaphore_signal(
                    barrier,
                    inc=1,
                    device_id=(lax.rem(g + dg, n_gr), f, lax.rem(t + dt, n_tp)),
                    device_id_type=MESH,
                )

    for near in (lax.rem(f + 1, n_fs), lax.rem(f + n_fs - 1, n_fs)):
        pl.semaphore_signal(barrier, inc=1, device_id=(g, near, t), device_id_type=MESH)
    pl.semaphore_wait(barrier, n_gr * n_tp + 1)

    outs = (gate_out, up_out)

    def held(o):
        return jnp.logical_and(o >= first, o < first + per)

    def block(m, o):
        if m < 2:
            return place(outs[m], g * n_fs + o)
        return down_out.at[o - first]

    def line(m, way, s):
        step = 1 if way == 0 else -1
        o = f - step * (s - 1)
        return pltpu.make_async_remote_copy(
            src_ref=block(m, o),
            dst_ref=block(m, o),
            send_sem=line_send.at[m, way, s],
            recv_sem=line_recv.at[m, way, s],
            device_id=(g, f + step, t),
            device_id_type=MESH,
        )

    def sends(m, way, s):
        step = 1 if way == 0 else -1
        o = f - step * (s - 1)
        fine = (f < n_fs - 1, o >= 0) if way == 0 else (f > 0, o <= n_fs - 1)
        ok = jnp.logical_and(*fine)
        return jnp.logical_and(ok, held(o)) if m == 2 else ok

    def gets(m, way, s):
        o = f - s if way == 0 else f + s
        ok = o >= 0 if way == 0 else o <= n_fs - 1
        return jnp.logical_and(ok, held(o)) if m == 2 else ok

    def landed(m, way, s):
        o = f - s if way == 0 else f + s
        return pltpu.make_async_remote_copy(
            src_ref=block(m, o),
            dst_ref=block(m, o),
            send_sem=line_send.at[m, way, s],
            recv_sem=line_recv.at[m, way, s],
            device_id=(g, f, t),
            device_id_type=MESH,
        )

    def pair(m, dg, o):
        return pltpu.make_async_remote_copy(
            src_ref=place(outs[m], g * n_fs + o),
            dst_ref=place(outs[m], g * n_fs + o),
            send_sem=pair_send.at[m, dg, o],
            recv_sem=pair_recv.at[m, dg, o],
            device_id=(lax.rem(g + dg, n_gr), f, t),
            device_id_type=MESH,
        )

    def pair_landed(m, dg, o):
        src = lax.rem(g - dg + n_gr, n_gr)
        return pltpu.make_async_remote_copy(
            src_ref=place(outs[m], src * n_fs + o),
            dst_ref=place(outs[m], src * n_fs + o),
            send_sem=pair_send.at[m, dg, o],
            recv_sem=pair_recv.at[m, dg, o],
            device_id=(src, f, t),
            device_id_type=MESH,
        )

    def part(dg):
        to = lax.rem(g + dg, n_gr)
        return pltpu.make_async_remote_copy(
            src_ref=down_own,
            dst_ref=down_out.at[slot, :, pl.ds(pl.multiple_of(t * cols, 128), cols)],
            send_sem=part_send.at[dg],
            recv_sem=part_recv.at[t],
            device_id=(to, f, owner),
            device_id_type=MESH,
        )

    def part_landed(src):
        return pltpu.make_async_remote_copy(
            src_ref=down_own,
            dst_ref=down_out.at[f - first, :, pl.ds(src * cols, cols)],
            send_sem=part_send.at[0],
            recv_sem=part_recv.at[src],
            device_id=(home, f, src),
            device_id_type=MESH,
        )

    for m in range(2):
        for way in range(2):

            @pl.when(sends(m, way, 1))
            def _(m=m, way=way):
                line(m, way, 1).start()

        for dg in range(1, n_gr):
            pair(m, dg, f).start()
    for dg in range(n_gr):
        if dg == 0:

            @pl.when(owner != t)
            def _():
                part(0).start()

        else:
            part(dg).start()

    @pl.when(held(f))
    def _():
        for src in range(n_tp):

            @pl.when(jnp.logical_or(home != g, t != src))
            def _(src=src):
                part_landed(src).wait_recv()

    for way in range(2):

        @pl.when(sends(2, way, 1))
        def _(way=way):
            line(2, way, 1).start()

    for s in range(1, n_fs):
        for m in range(3):
            for way in range(2):

                @pl.when(gets(m, way, s))
                def _(m=m, way=way, s=s):
                    landed(m, way, s).wait_recv()
                    if s < n_fs - 1:

                        @pl.when(sends(m, way, s + 1))
                        def _():
                            line(m, way, s + 1).start()

                    if m < 2:
                        o = f - s if way == 0 else f + s
                        for dg in range(1, n_gr):
                            pair(m, dg, o).start()

    for m in range(2):
        for dg in range(1, n_gr):
            for o in range(n_fs):
                pair_landed(m, dg, o).wait_recv()
                pair(m, dg, o).wait_send()
    for m in range(3):
        for way in range(2):
            for s in range(1, n_fs):

                @pl.when(sends(m, way, s))
                def _(m=m, way=way, s=s):
                    line(m, way, s).wait_send()

    for dg in range(n_gr):
        if dg == 0:

            @pl.when(owner != t)
            def _():
                part(0).wait_send()

        else:
            part(dg).wait_send()


def gather(sizes, call, gain, gate, up, down):
    n_gr, n_fs, n_tp = sizes
    per = n_gr * n_fs // n_tp
    rows, width = gate.shape
    wide = rows % 128 == 0
    whole = (width, n_gr * n_fs * rows) if wide else (n_gr * n_fs, width, rows)
    tall, cols = down.shape
    vmem = pl.BlockSpec(memory_space=pltpu.VMEM)
    dma = pltpu.SemaphoreType.DMA
    gate_all, up_all, down_all = pl.pallas_call(
        functools.partial(gather_kernel, n_gr, n_fs, n_tp),
        out_shape=(
            jax.ShapeDtypeStruct(whole, jnp.bfloat16),
            jax.ShapeDtypeStruct(whole, jnp.bfloat16),
            jax.ShapeDtypeStruct((per, tall, n_tp * cols), jnp.bfloat16),
        ),
        in_specs=[vmem] * 4,
        out_specs=(vmem,) * 3,
        scratch_shapes=[
            pltpu.VMEM((tall, cols), jnp.bfloat16),
            dma((3, 2, n_fs)),
            dma((3, 2, n_fs)),
            dma((2, n_gr, n_fs)),
            dma((2, n_gr, n_fs)),
            dma((n_gr,)),
            dma((n_tp,)),
        ],
        compiler_params=pltpu.CompilerParams(
            collective_id=call, has_side_effects=True, vmem_limit_bytes=32 * 2**20
        ),
        cost_estimate=pl.CostEstimate(
            flops=10**10, bytes_accessed=16 * 2**20, transcendentals=0
        ),
    )(gain[None, :], gate.T, up.T, down)

    def upright(a):
        return a.T if wide else a.transpose(0, 2, 1).reshape(n_gr * n_fs * rows, width)

    return (
        upright(gate_all),
        upright(up_all),
        down_all.reshape(per * tall, n_tp * cols),
    )


def fused_kernel(
    n_gr,
    n_fs,
    n_tp,
    prompt_in,
    gain_in_a,
    gate_in_a,
    up_in_a,
    down_in_a,
    gain_in_b,
    gate_in_b,
    up_in_b,
    down_in_b,
    gate_out_a,
    up_out_a,
    down_out_a,
    gate_out_b,
    up_out_b,
    down_out_b,
    mixed_ref,
    prompt,
    gains,
    tall_in,
    gates_in,
    load_sem,
    down_own,
    normed,
    normed_all,
    hidden,
    mate_out,
    mate_in,
    sums,
    sums_in,
    kept,
    stream,
    line_send,
    line_recv,
    pair_send,
    pair_recv,
    part_send,
    part_recv,
    mate_send,
    mate_recv,
    sum_send,
    sum_recv,
    row_send,
    row_recv,
):
    g, f, t = lax.axis_index("gr"), lax.axis_index("fs"), lax.axis_index("tp")
    per = n_gr * n_fs // n_tp
    tall, cols = down_in_a.shape
    width = gate_in_a.shape[1]
    owned, depth = prompt.shape[1], prompt.shape[2]
    first = lax.rem(t * per, n_fs)
    home = (t * per) // n_fs
    row = g * n_fs + f
    owner = row // per
    slot = lax.rem(row, per)
    pairs = n_tp // 2
    seat, core = t // 2, lax.rem(t, 2)
    outs = ((gate_out_a, up_out_a, down_out_a), (gate_out_b, up_out_b, down_out_b))

    half, quarter, eighth = depth // 2, depth // 4, depth // 8

    def lanes(at, size):
        return pl.ds(pl.multiple_of(at, 128), size)

    def crossed(column, i):
        return half + column * quarter + i * eighth

    shared = ((0, quarter), (quarter, eighth), (quarter + eighth, eighth))
    carried = 2 + 2
    count = carried + len(shared)

    loads = []
    for k, (src, dst) in enumerate(
        (
            (gain_in_a, gains.at[0]),
            (gate_in_a, gates_in.at[0]),
            (up_in_a, gates_in.at[1]),
            (down_in_a, tall_in.at[0]),
            (prompt_in, prompt),
            (gain_in_b, gains.at[1]),
            (down_in_b, tall_in.at[1]),
            (gate_in_b, gates_in.at[2]),
            (up_in_b, gates_in.at[3]),
        )
    ):
        load = pltpu.make_async_copy(src, dst, load_sem.at[k])
        load.start()
        loads.append(load)

    barrier = pltpu.get_barrier_semaphore()
    for dg in range(n_gr):
        for dt in range(n_tp):
            if dg or dt:
                pl.semaphore_signal(
                    barrier,
                    inc=1,
                    device_id=(lax.rem(g + dg, n_gr), f, lax.rem(t + dt, n_tp)),
                    device_id_type=MESH,
                )
    for near in (lax.rem(f + 1, n_fs), lax.rem(f + n_fs - 1, n_fs)):
        pl.semaphore_signal(barrier, inc=1, device_id=(g, near, t), device_id_type=MESH)

    def place(ref, origin):
        return ref.at[:, pl.ds(pl.multiple_of(origin * width, 128), width)]

    def round_matrix(n, m):
        place(outs[n][m], row)[...] = (gains[n] * gates_in[2 * n + m]).astype(jnp.bfloat16)

    def round_down(n):
        rounded = tall_in[n].astype(jnp.bfloat16)
        down_own[n] = rounded

        @pl.when(owner == t)
        def _():
            outs[n][2][slot, :, lanes(t * cols, cols)] = rounded

    def held(o):
        return jnp.logical_and(o >= first, o < first + per)

    def remote(src, dst, send, recv, to):
        return pltpu.make_async_remote_copy(
            src_ref=src,
            dst_ref=dst,
            send_sem=send,
            recv_sem=recv,
            device_id=to,
            device_id_type=MESH,
        )

    def spot(n, p, o, column):
        if p < 2:
            return place(outs[n][p], column * n_fs + o)
        if p < carried:
            at, size = crossed(column, p - 2), eighth
        else:
            at, size = shared[p - carried]
        return outs[n][2].at[o - first, :, lanes(at, size)]

    def line(n, p, way, s):
        step = 1 if way == 0 else -1
        o = f - step * (s - 1)
        sems = line_send.at[n, p, way, s], line_recv.at[n, p, way, s]
        return remote(spot(n, p, o, g), spot(n, p, o, g), *sems, (g, f + step, t))

    def sends(p, way, s):
        step = 1 if way == 0 else -1
        o = f - step * (s - 1)
        fine = (f < n_fs - 1, o >= 0) if way == 0 else (f > 0, o <= n_fs - 1)
        ok = jnp.logical_and(*fine)
        return jnp.logical_and(ok, held(o)) if p >= 2 else ok

    def origin(way, s):
        return f - s if way == 0 else f + s

    def gets(p, way, s):
        o = origin(way, s)
        ok = o >= 0 if way == 0 else o <= n_fs - 1
        return jnp.logical_and(ok, held(o)) if p >= 2 else ok

    def ends(way):
        return f == n_fs - 1 if way == 0 else f == 0

    def landed(n, p, way, s):
        o = origin(way, s)
        sems = line_send.at[n, p, way, s], line_recv.at[n, p, way, s]
        return remote(spot(n, p, o, g), spot(n, p, o, g), *sems, (g, f, t))

    def pair(n, p, o):
        sems = pair_send.at[n, p, o], pair_recv.at[n, p, o]
        return remote(spot(n, p, o, g), spot(n, p, o, g), *sems, (1 - g, f, t))

    def pair_landed(n, p, o):
        sems = pair_send.at[n, p, o], pair_recv.at[n, p, o]
        return remote(spot(n, p, o, 1 - g), spot(n, p, o, 1 - g), *sems, (1 - g, f, t))

    def part(n, dg):
        return remote(
            down_own.at[n],
            outs[n][2].at[slot, :, lanes(t * cols, cols)],
            part_send.at[n, dg],
            part_recv.at[n, t],
            (lax.rem(g + dg, n_gr), f, owner),
        )

    def part_landed(n, src):
        return remote(
            down_own.at[n],
            outs[n][2].at[f - first, :, pl.ds(src * cols, cols)],
            part_send.at[n, 0],
            part_recv.at[n, src],
            (home, f, src),
        )

    def start_lines(n, p):
        for way in range(2):

            @pl.when(sends(p, way, 1))
            def _(way=way):
                line(n, p, way, 1).start()

    def give_part(n):
        @pl.when(owner != t)
        def _():
            part(n, 0).start()

    def start_down(n):
        @pl.when(held(f))
        def _():
            for src in range(n_tp):

                @pl.when(jnp.logical_or(home != g, t != src))
                def _(src=src):
                    part_landed(n, src).wait_recv()

        for p in range(2, count):
            start_lines(n, p)

    def forward(n, p, s):
        crosses, relays = p < carried, s < n_fs - 1
        for way in range(2):
            if not crosses and not relays:
                continue
            ready = gets(p, way, s)
            if not crosses:
                ready = jnp.logical_and(ready, jnp.logical_not(ends(way)))

            @pl.when(ready)
            def _(way=way):
                landed(n, p, way, s).wait_recv()
                if relays:

                    @pl.when(sends(p, way, s + 1))
                    def _():
                        line(n, p, way, s + 1).start()

                if crosses:
                    pair(n, p, origin(way, s)).start()

    def settle(n, p):
        for s in range(1, n_fs):
            for way in range(2):
                ready = gets(p, way, s)
                if s < n_fs - 1:
                    ready = jnp.logical_and(ready, ends(way))

                @pl.when(ready)
                def _(way=way, s=s):
                    landed(n, p, way, s).wait_recv()

    def pairs_in(n, p):
        for o in range(n_fs):
            if p < 2:
                pair_landed(n, p, o).wait_recv()
            else:

                @pl.when(jnp.logical_and(held(o), o != f))
                def _(o=o):
                    pair_landed(n, p, o).wait_recv()

    def drain(n):
        for p in range(carried):
            for o in range(n_fs):
                if p < 2:
                    pair(n, p, o).wait_send()
                else:

                    @pl.when(jnp.logical_and(held(o), o != f))
                    def _(p=p, o=o):
                        pair(n, p, o).wait_send()

        for p in range(count):
            for way in range(2):
                for s in range(1, n_fs):

                    @pl.when(sends(p, way, s))
                    def _(p=p, way=way, s=s):
                        line(n, p, way, s).wait_send()

        @pl.when(owner != t)
        def _():
            part(n, 0).wait_send()

        part(n, 1).wait_send()

    across = (((1,), (1,)), ((), ()))

    def unit(rows):
        return rows * lax.rsqrt(jnp.mean(rows * rows, axis=-1, keepdims=True) + 1e-06)

    def seat_of(j):
        return lax.rem(seat + 1 + j, pairs)

    def hide(n, source):
        @pl.loop(0, 2)
        def _(c):
            rows = jnp.concatenate([source[c, seat_of(j)] for j in range(pairs)], axis=0)
            gate = lax.dot_general(
                rows, outs[n][0][...], across, preferred_element_type=jnp.float32
            )
            upper = lax.dot_general(
                rows, outs[n][1][...], across, preferred_element_type=jnp.float32
            )
            hidden[c] = (jax.nn.silu(gate) * upper).astype(jnp.bfloat16)

    ranges = (
        ((crossed(g, 0), quarter),),
        ((0, quarter),),
        ((quarter, eighth), (crossed(1 - g, 0), eighth)),
        ((quarter + eighth, eighth), (crossed(1 - g, 1), eighth)),
    )
    steps = len(ranges)
    span = depth // steps

    def mate(n, k):
        at = pl.ds(k * span, span)
        return remote(
            mate_out.at[n, :, at],
            mate_in.at[n, :, at],
            mate_send.at[n, k],
            mate_recv.at[n, k],
            (g, f, t + 1 - 2 * core),
        )

    def share(n, k, j):
        at = pl.ds(k * span, span)
        return remote(
            sums.at[n, j, :, at],
            sums_in.at[n, j, :, at],
            sum_send.at[n, k, j],
            sum_recv.at[n, k, j],
            (g, f, 2 * seat_of(j) + core),
        )

    def term(n, units, k):
        tiles = [
            jnp.dot(
                units,
                outs[n][2][:, :, lanes(at, size)].reshape(per * tall, size),
                preferred_element_type=jnp.float32,
            )
            for at, size in ranges[k]
        ]
        return tiles[0] if len(tiles) == 1 else jnp.concatenate(tiles, axis=1)

    def offer(n, k):
        mate_out[n, :, pl.ds(k * span, span)] = term(n, hidden[1 - core], k).astype(jnp.bfloat16)
        mate(n, k).start()

    def reduce(n, k):
        at = pl.ds(k * span, span)
        mine = term(n, hidden[core], k)
        mate(n, k).wait_recv()
        both = mine + mate_in[n, :, at].astype(jnp.float32)
        for j in range(pairs - 1):
            sums[n, j, :, at] = both[j * owned : (j + 1) * owned].astype(jnp.bfloat16)
            share(n, k, j).start()
        kept[:, at] = both[(pairs - 1) * owned :]

    def collect(n, k, base, finish):
        for j in range(pairs - 1):
            share(n, k, j).wait_recv()
        total = kept[:, pl.ds(k * span, span)]
        for j in range(pairs - 1):
            total += sums_in[n, j, :, pl.ds(k * span, span)].astype(jnp.float32)
        passed = 0
        for at, size in ranges[k]:
            finish(lanes(at, size), base(lanes(at, size)) + 0.5 * total[:, passed : passed + size])
            passed += size

    def give(j):
        own = normed_all.at[core, seat]
        return remote(own, own, row_send.at[j], row_recv.at[j], (g, f, 2 * seat_of(j) + core))

    def given(j):
        src = lax.rem(seat - 1 - j + pairs, pairs)
        spot = normed_all.at[core, src]
        return remote(spot, spot, row_send.at[j], row_recv.at[j], (g, f, 2 * src + core))

    def pass_on(j):
        src = lax.rem(seat - 1 - j + 2 * pairs, pairs)
        spot = normed_all.at[core, src]
        at = pairs - 1 + (pairs - 1 if j < 0 else j)
        return remote(
            spot, spot, row_send.at[at], row_recv.at[at], (g, f, t + 1 - 2 * core)
        )

    def passed_on(j):
        src = lax.rem(seat - 1 - j + 2 * pairs, pairs)
        spot = normed_all.at[1 - core, src]
        at = pairs - 1 + (pairs - 1 if j < 0 else j)
        return remote(
            spot, spot, row_send.at[at], row_recv.at[at], (g, f, t + 1 - 2 * core)
        )

    loads[0].wait()
    loads[1].wait()
    round_matrix(0, 0)
    pl.semaphore_wait(barrier, n_gr * n_tp + 1)
    start_lines(0, 0)
    pair(0, 0, f).start()
    loads[2].wait()
    round_matrix(0, 1)
    start_lines(0, 1)
    pair(0, 1, f).start()
    loads[3].wait()
    round_down(0)
    part(0, 1).start()
    give_part(0)
    loads[5].wait()
    loads[6].wait()
    round_down(1)
    give_part(1)
    loads[7].wait()
    round_matrix(1, 0)
    loads[8].wait()
    round_matrix(1, 1)
    loads[4].wait()

    @pl.loop(0, n_tp)
    def _(i):
        normed[lax.rem(i, 2), i // 2] = unit(prompt[i].astype(jnp.float32)).astype(jnp.bfloat16)

    def first_half(n):
        for m in range(2):
            forward(n, m, 1)

    def second_half(n):
        for s in range(2, n_fs):
            for m in range(2):
                forward(n, m, s)
            if s == 2:
                start_down(n)

    def downs(n):
        for p in range(2, carried):
            for s in range(1, n_fs):
                forward(n, p, s)
        for p in range(carried, count):
            for s in range(1, n_fs):
                forward(n, p, s)

    first_half(0)
    second_half(0)
    downs(0)
    part(1, 1).start()
    for m in range(2):
        start_lines(1, m)
        pair(1, m, f).start()
    for m in range(2):
        pairs_in(0, m)
    hide(0, normed)
    settle(0, carried)
    offer(0, 0)
    offer(0, 1)
    reduce(0, 0)
    reduce(0, 1)
    for k in range(2, steps):
        settle(0, carried + k - 1)
        pairs_in(0, k)
        offer(0, k)
    for k in range(2, steps):
        reduce(0, k)
    first_half(1)

    def own_prompt(at):
        return prompt[t, :, at].astype(jnp.float32)

    def keep_stream(at, value):
        stream[:, at] = value

    for k in range(steps):
        collect(0, k, own_prompt, keep_stream)
    normed_all[core, seat] = unit(stream[...]).astype(jnp.bfloat16)
    for j in range(pairs - 1):
        give(j).start()
    pass_on(-1).start()
    for s in range(2, n_fs):
        for m in range(2):
            forward(1, m, s)
        if s == 2:
            start_down(1)
            for j in range(pairs - 1):
                given(j).wait_recv()
                pass_on(j).start()
    downs(1)
    for j in range(-1, pairs - 1):
        passed_on(j).wait_recv()
    for m in range(2):
        pairs_in(1, m)
    hide(1, normed_all)

    def keep_mixed(at, value):
        mixed_ref[:, at] = value.astype(jnp.bfloat16)

    def own_stream(at):
        return stream[:, at]

    offer(1, 0)
    settle(1, carried)
    offer(1, 1)
    reduce(1, 0)
    reduce(1, 1)
    for k in range(2, steps):
        settle(1, carried + k - 1)
        pairs_in(1, k)
        offer(1, k)
        reduce(1, k)
    drain(0)
    drain(1)
    for k in range(steps):
        collect(1, k, own_stream, keep_mixed)
    for j in range(pairs - 1):
        give(j).wait_send()
    for j in range(-1, pairs - 1):
        pass_on(j).wait_send()
    for n in range(2):
        for k in range(steps):
            mate(n, k).wait_send()
            for j in range(pairs - 1):
                share(n, k, j).wait_send()


def write_kernel(*refs):
    count = (len(refs) - 1) // 2
    sems = refs[-1]
    copies = [
        pltpu.make_async_copy(refs[k], refs[count + k], sems.at[k]) for k in range(count)
    ]
    for copy in copies:
        copy.start()
    for copy in copies:
        copy.wait()


def written(arrays):
    arrays = [pltpu.with_memory_space_constraint(a, pltpu.VMEM) for a in arrays]
    return pl.pallas_call(
        write_kernel,
        out_shape=tuple(jax.ShapeDtypeStruct(a.shape, a.dtype) for a in arrays),
        in_specs=[pl.BlockSpec(memory_space=pltpu.VMEM)] * len(arrays),
        out_specs=(pl.BlockSpec(memory_space=pl.ANY),) * len(arrays),
        scratch_shapes=[pltpu.SemaphoreType.DMA((len(arrays),))],
        compiler_params=pltpu.CompilerParams(vmem_limit_bytes=2**20),
    )(*arrays)


def fused(sizes, prompt, *weights):
    n_gr, n_fs, n_tp = sizes
    per = n_gr * n_fs // n_tp
    tokens, depth = prompt.shape
    owned = tokens // n_tp
    rows, width = weights[1].shape
    tall, cols = weights[3].shape
    pairs = n_tp // 2
    steps, pieces = 4, 7
    vmem = pl.BlockSpec(memory_space=pltpu.VMEM)
    hbm = pl.BlockSpec(memory_space=pltpu.HBM)
    dma = pltpu.SemaphoreType.DMA
    across = pltpu.VMEM((width, n_gr * n_fs * rows), jnp.bfloat16)
    down = pltpu.VMEM((per, tall, n_tp * cols), jnp.bfloat16)
    operands = [prompt.reshape(n_tp, owned, depth)]
    for n in range(2):
        gain, gate, up, tall_block = weights[4 * n : 4 * n + 4]
        operands += [gain[None, :], gate.T, up.T, tall_block]
    results = pl.pallas_call(
        functools.partial(fused_kernel, n_gr, n_fs, n_tp),
        out_shape=(across, across, down) * 2 + (pltpu.VMEM((owned, depth), jnp.bfloat16),),
        in_specs=[hbm] * 9,
        out_specs=(vmem,) * 7,
        scratch_shapes=[
            pltpu.VMEM((n_tp, owned, depth), prompt.dtype),
            pltpu.VMEM((2, 1, rows), jnp.float32),
            pltpu.VMEM((2, tall, cols), jnp.float32),
            pltpu.VMEM((4, width, rows), jnp.float32),
            dma((9,)),
            pltpu.VMEM((2, tall, cols), jnp.bfloat16),
            pltpu.VMEM((2, pairs, owned, depth), jnp.bfloat16),
            pltpu.VMEM((2, pairs, owned, depth), jnp.bfloat16),
            pltpu.VMEM((2, pairs * owned, width), jnp.bfloat16),
            pltpu.VMEM((2, pairs * owned, depth), jnp.bfloat16),
            pltpu.VMEM((2, pairs * owned, depth), jnp.bfloat16),
            pltpu.VMEM((2, pairs - 1, owned, depth), jnp.bfloat16),
            pltpu.VMEM((2, pairs - 1, owned, depth), jnp.bfloat16),
            pltpu.VMEM((owned, depth), jnp.float32),
            pltpu.VMEM((owned, depth), jnp.float32),
            dma((2, pieces, 2, n_fs)),
            dma((2, pieces, 2, n_fs)),
            dma((2, 4, n_fs)),
            dma((2, 4, n_fs)),
            dma((2, n_gr)),
            dma((2, n_tp)),
            dma((2, steps)),
            dma((2, steps)),
            dma((2, steps, pairs - 1)),
            dma((2, steps, pairs - 1)),
            dma((2 * pairs - 1,)),
            dma((2 * pairs - 1,)),
        ],
        compiler_params=pltpu.CompilerParams(
            collective_id=2, has_side_effects=True, vmem_limit_bytes=36 * 2**20
        ),
    )(*operands)
    gate_a, up_a, down_a, gate_b, up_b, down_b, mixed = written(results)

    def flat(a):
        return a.reshape(per * tall, n_tp * cols)

    return (gate_a.T, up_a.T, flat(down_a), gate_b.T, up_b.T, flat(down_b), mixed)


def normalize(rows):
    rows = rows.astype(jnp.float32)
    scale = lax.rsqrt(jnp.mean(rows * rows, axis=-1, keepdims=True) + 1e-06)
    return (rows * scale).astype(jnp.bfloat16)


def hidden_units(normed, w_gate, w_up):
    gate = jnp.dot(normed, w_gate, preferred_element_type=jnp.float32)
    upper = jnp.dot(normed, w_up, preferred_element_type=jnp.float32)
    return (jax.nn.silu(gate) * upper).astype(jnp.bfloat16)


def rounded_term(hidden, w_down):
    return jnp.dot(hidden, w_down, preferred_element_type=jnp.float32).astype(jnp.bfloat16)


def suits(sizes, prompt, gate, down):
    n_gr, n_fs, n_tp = sizes
    per = n_gr * n_fs // n_tp
    return (
        n_gr == 2
        and n_tp % 2 == 0
        and per > 0
        and per * n_tp == n_gr * n_fs
        and n_fs % per == 0
        and gate.shape[0] % 128 == 0
        and down.shape[0] % 16 == 0
        and down.shape[1] % 128 == 0
        and prompt.shape[1] % 1024 == 0
        and prompt.shape[0] % (16 * n_tp) == 0
    )


def shards(
    sizes,
    prompt,
    gain_first,
    gate_first,
    up_first,
    down_first,
    gain_second,
    gate_second,
    up_second,
    down_second,
):
    if suits(sizes, prompt, gate_first, down_first):
        return fused(
            sizes,
            prompt,
            gain_first,
            gate_first,
            up_first,
            down_first,
            gain_second,
            gate_second,
            up_second,
            down_second,
        )
    gate_a, up_a, down_a = gather(sizes, 0, gain_first, gate_first, up_first, down_first)
    hidden_a = hidden_units(normalize(prompt), gate_a, up_a)
    term_a = rounded_term(hidden_a, down_a)
    term_a, gain_second = lax.optimization_barrier((term_a, gain_second))
    branch_a = lax.psum(term_a, "tp").astype(jnp.float32)
    gate_b, up_b, down_b = gather(sizes, 1, gain_second, gate_second, up_second, down_second)
    stream = prompt.astype(jnp.float32) + 0.5 * branch_a
    hidden_b = hidden_units(normalize(stream), gate_b, up_b)
    owned = hidden_b.shape[0] // lax.axis_size("tp")
    branch_b = lax.psum_scatter(
        rounded_term(hidden_b, down_b), "tp", scatter_dimension=0, tiled=True
    ).astype(jnp.float32)
    own_stream = lax.dynamic_slice_in_dim(stream, lax.axis_index("tp") * owned, owned, 0)
    mixed = (own_stream + 0.5 * branch_b).astype(jnp.bfloat16)
    return (gate_a, up_a, down_a, gate_b, up_b, down_b, mixed)


def solution(mesh):
    sizes = (mesh.shape["gr"], mesh.shape["fs"], mesh.shape["tp"])
    return jax.shard_map(
        functools.partial(shards, sizes),
        mesh=mesh,
        in_specs=(
            P(("gr", "fs"), None),
            P(("gr", "fs")),
            P(("gr", "fs"), "tp"),
            P(("gr", "fs"), "tp"),
            P(("gr", "fs"), "tp"),
            P(("gr", "fs")),
            P(("gr", "fs"), "tp"),
            P(("gr", "fs"), "tp"),
            P(("gr", "fs"), "tp"),
        ),
        out_specs=(
            P(None, "tp"),
            P(None, "tp"),
            P("tp", None),
            P(None, "tp"),
            P(None, "tp"),
            P("tp", None),
            P(("gr", "fs", "tp"), None),
        ),
        check_vma=False,
    )
```

```python
import functools

import jax
import jax.numpy as jnp
from jax import lax
from jax.experimental import pallas as pl
from jax.experimental.pallas import tpu as pltpu
from jax.sharding import PartitionSpec as P

MESH = pl.DeviceIdType.MESH


def gather_kernel(
    n_gr,
    n_fs,
    n_tp,
    gain_ref,
    gate_ref,
    up_ref,
    down_ref,
    gate_out,
    up_out,
    down_out,
    down_own,
    line_send,
    line_recv,
    pair_send,
    pair_recv,
    part_send,
    part_recv,
):
    g, f, t = lax.axis_index("gr"), lax.axis_index("fs"), lax.axis_index("tp")
    per = n_gr * n_fs // n_tp
    cols = down_ref.shape[1]
    first = lax.rem(t * per, n_fs)
    home = (t * per) // n_fs
    row = g * n_fs + f
    owner = row // per
    slot = lax.rem(row, per)

    width = gate_ref.shape[1]

    def place(ref, origin):
        if len(ref.shape) == 3:
            return ref.at[origin]
        return ref.at[:, pl.ds(pl.multiple_of(origin * width, 128), width)]

    gain = gain_ref[...]
    place(gate_out, row)[...] = (gain * gate_ref[...]).astype(jnp.bfloat16)
    place(up_out, row)[...] = (gain * up_ref[...]).astype(jnp.bfloat16)
    down_own[...] = down_ref[...].astype(jnp.bfloat16)

    @pl.when(owner == t)
    def _():
        down_out[slot, :, pl.ds(pl.multiple_of(t * cols, 128), cols)] = down_ref[...].astype(
            jnp.bfloat16
        )

    barrier = pltpu.get_barrier_semaphore()
    for dg in range(n_gr):
        for dt in range(n_tp):
            if dg or dt:
                pl.semaphore_signal(
                    barrier,
                    inc=1,
                    device_id=(lax.rem(g + dg, n_gr), f, lax.rem(t + dt, n_tp)),
                    device_id_type=MESH,
                )

    for near in (lax.rem(f + 1, n_fs), lax.rem(f + n_fs - 1, n_fs)):
        pl.semaphore_signal(barrier, inc=1, device_id=(g, near, t), device_id_type=MESH)
    pl.semaphore_wait(barrier, n_gr * n_tp + 1)

    outs = (gate_out, up_out)

    def held(o):
        return jnp.logical_and(o >= first, o < first + per)

    def block(m, o):
        if m < 2:
            return place(outs[m], g * n_fs + o)
        return down_out.at[o - first]

    def line(m, way, s):
        step = 1 if way == 0 else -1
        o = f - step * (s - 1)
        return pltpu.make_async_remote_copy(
            src_ref=block(m, o),
            dst_ref=block(m, o),
            send_sem=line_send.at[m, way, s],
            recv_sem=line_recv.at[m, way, s],
            device_id=(g, f + step, t),
            device_id_type=MESH,
        )

    def sends(m, way, s):
        step = 1 if way == 0 else -1
        o = f - step * (s - 1)
        fine = (f < n_fs - 1, o >= 0) if way == 0 else (f > 0, o <= n_fs - 1)
        ok = jnp.logical_and(*fine)
        return jnp.logical_and(ok, held(o)) if m == 2 else ok

    def gets(m, way, s):
        o = f - s if way == 0 else f + s
        ok = o >= 0 if way == 0 else o <= n_fs - 1
        return jnp.logical_and(ok, held(o)) if m == 2 else ok

    def landed(m, way, s):
        o = f - s if way == 0 else f + s
        return pltpu.make_async_remote_copy(
            src_ref=block(m, o),
            dst_ref=block(m, o),
            send_sem=line_send.at[m, way, s],
            recv_sem=line_recv.at[m, way, s],
            device_id=(g, f, t),
            device_id_type=MESH,
        )

    def pair(m, dg, o):
        return pltpu.make_async_remote_copy(
            src_ref=place(outs[m], g * n_fs + o),
            dst_ref=place(outs[m], g * n_fs + o),
            send_sem=pair_send.at[m, dg, o],
            recv_sem=pair_recv.at[m, dg, o],
            device_id=(lax.rem(g + dg, n_gr), f, t),
            device_id_type=MESH,
        )

    def pair_landed(m, dg, o):
        src = lax.rem(g - dg + n_gr, n_gr)
        return pltpu.make_async_remote_copy(
            src_ref=place(outs[m], src * n_fs + o),
            dst_ref=place(outs[m], src * n_fs + o),
            send_sem=pair_send.at[m, dg, o],
            recv_sem=pair_recv.at[m, dg, o],
            device_id=(src, f, t),
            device_id_type=MESH,
        )

    def part(dg):
        to = lax.rem(g + dg, n_gr)
        return pltpu.make_async_remote_copy(
            src_ref=down_own,
            dst_ref=down_out.at[slot, :, pl.ds(pl.multiple_of(t * cols, 128), cols)],
            send_sem=part_send.at[dg],
            recv_sem=part_recv.at[t],
            device_id=(to, f, owner),
            device_id_type=MESH,
        )

    def part_landed(src):
        return pltpu.make_async_remote_copy(
            src_ref=down_own,
            dst_ref=down_out.at[f - first, :, pl.ds(src * cols, cols)],
            send_sem=part_send.at[0],
            recv_sem=part_recv.at[src],
            device_id=(home, f, src),
            device_id_type=MESH,
        )

    for m in range(2):
        for way in range(2):

            @pl.when(sends(m, way, 1))
            def _(m=m, way=way):
                line(m, way, 1).start()

        for dg in range(1, n_gr):
            pair(m, dg, f).start()
    for dg in range(n_gr):
        if dg == 0:

            @pl.when(owner != t)
            def _():
                part(0).start()

        else:
            part(dg).start()

    @pl.when(held(f))
    def _():
        for src in range(n_tp):

            @pl.when(jnp.logical_or(home != g, t != src))
            def _(src=src):
                part_landed(src).wait_recv()

    for way in range(2):

        @pl.when(sends(2, way, 1))
        def _(way=way):
            line(2, way, 1).start()

    for s in range(1, n_fs):
        for m in range(3):
            for way in range(2):

                @pl.when(gets(m, way, s))
                def _(m=m, way=way, s=s):
                    landed(m, way, s).wait_recv()
                    if s < n_fs - 1:

                        @pl.when(sends(m, way, s + 1))
                        def _():
                            line(m, way, s + 1).start()

                    if m < 2:
                        o = f - s if way == 0 else f + s
                        for dg in range(1, n_gr):
                            pair(m, dg, o).start()

    for m in range(2):
        for dg in range(1, n_gr):
            for o in range(n_fs):
                pair_landed(m, dg, o).wait_recv()
                pair(m, dg, o).wait_send()
    for m in range(3):
        for way in range(2):
            for s in range(1, n_fs):

                @pl.when(sends(m, way, s))
                def _(m=m, way=way, s=s):
                    line(m, way, s).wait_send()

    for dg in range(n_gr):
        if dg == 0:

            @pl.when(owner != t)
            def _():
                part(0).wait_send()

        else:
            part(dg).wait_send()


def gather(sizes, call, gain, gate, up, down):
    n_gr, n_fs, n_tp = sizes
    per = n_gr * n_fs // n_tp
    rows, width = gate.shape
    wide = rows % 128 == 0
    whole = (width, n_gr * n_fs * rows) if wide else (n_gr * n_fs, width, rows)
    tall, cols = down.shape
    vmem = pl.BlockSpec(memory_space=pltpu.VMEM)
    dma = pltpu.SemaphoreType.DMA
    gate_all, up_all, down_all = pl.pallas_call(
        functools.partial(gather_kernel, n_gr, n_fs, n_tp),
        out_shape=(
            jax.ShapeDtypeStruct(whole, jnp.bfloat16),
            jax.ShapeDtypeStruct(whole, jnp.bfloat16),
            jax.ShapeDtypeStruct((per, tall, n_tp * cols), jnp.bfloat16),
        ),
        in_specs=[vmem] * 4,
        out_specs=(vmem,) * 3,
        scratch_shapes=[
            pltpu.VMEM((tall, cols), jnp.bfloat16),
            dma((3, 2, n_fs)),
            dma((3, 2, n_fs)),
            dma((2, n_gr, n_fs)),
            dma((2, n_gr, n_fs)),
            dma((n_gr,)),
            dma((n_tp,)),
        ],
        compiler_params=pltpu.CompilerParams(
            collective_id=call, has_side_effects=True, vmem_limit_bytes=32 * 2**20
        ),
        cost_estimate=pl.CostEstimate(
            flops=10**10, bytes_accessed=16 * 2**20, transcendentals=0
        ),
    )(gain[None, :], gate.T, up.T, down)

    def upright(a):
        return a.T if wide else a.transpose(0, 2, 1).reshape(n_gr * n_fs * rows, width)

    return (
        upright(gate_all),
        upright(up_all),
        down_all.reshape(per * tall, n_tp * cols),
    )


def down_pieces(depth):
    half, quarter, eighth, piece = depth // 2, depth // 4, depth // 8, depth // 16
    split = ((0, eighth), (eighth, piece), (eighth + piece, piece))
    shared = (
        (0, quarter),
        (quarter, eighth),
        (quarter + eighth, piece),
        (half - piece, piece),
    )
    groups = (((0,), ()), ((1,), (0,)), ((2,), (1,)), ((3,), (2,)))
    return split, shared, groups


def column_ranges(depth, g):
    split, shared, groups = down_pieces(depth)
    half, quarter = depth // 2, depth // 4
    ranges = [((half + g * quarter, quarter),)]
    for whole, pieces in groups:
        ranges.append(
            tuple(shared[i] for i in whole)
            + tuple((half + (1 - g) * quarter + split[i][0], split[i][1]) for i in pieces)
        )
    return ranges


INSIDE = 2


def fused_kernel(
    n_gr,
    n_fs,
    n_tp,
    prompt_in,
    gain_in_a,
    gate_in_a,
    up_in_a,
    down_in_a,
    gain_in_b,
    gate_in_b,
    up_in_b,
    down_in_b,
    gate_out_a,
    up_out_a,
    down_out_a,
    gate_out_b,
    up_out_b,
    down_out_b,
    mixed_ref,
    late_sums,
    late_rest,
    prompt,
    gains,
    tall_in,
    gates_in,
    load_sem,
    down_own,
    normed,
    normed_all,
    hidden,
    mate_out,
    mate_in,
    sums,
    sums_in,
    kept,
    stream,
    line_send,
    line_recv,
    pair_send,
    pair_recv,
    part_send,
    part_recv,
    mate_send,
    mate_recv,
    sum_send,
    sum_recv,
    row_send,
    row_recv,
):
    g, f, t = lax.axis_index("gr"), lax.axis_index("fs"), lax.axis_index("tp")
    per = n_gr * n_fs // n_tp
    tall, cols = down_in_a.shape
    width = gate_in_a.shape[1]
    owned, depth = prompt.shape[1], prompt.shape[2]
    first = lax.rem(t * per, n_fs)
    home = (t * per) // n_fs
    row = g * n_fs + f
    owner = row // per
    slot = lax.rem(row, per)
    pairs = n_tp // 2
    seat, core = t // 2, lax.rem(t, 2)
    outs = ((gate_out_a, up_out_a, down_out_a), (gate_out_b, up_out_b, down_out_b))

    split, shared, groups = down_pieces(depth)
    half, quarter = depth // 2, depth // 4
    carried = 2 + len(split)
    count = carried + len(shared)

    def lanes(at, size):
        return pl.ds(pl.multiple_of(at, 128), size)

    def crossed(column, i):
        at, size = split[i]
        return half + column * quarter + at, size

    loads = []
    for k, (src, dst) in enumerate(
        (
            (gain_in_a, gains.at[0]),
            (gate_in_a, gates_in.at[0]),
            (up_in_a, gates_in.at[1]),
            (down_in_a, tall_in.at[0]),
            (prompt_in, prompt),
            (gain_in_b, gains.at[1]),
            (down_in_b, tall_in.at[1]),
            (gate_in_b, gates_in.at[2]),
            (up_in_b, gates_in.at[3]),
        )
    ):
        load = pltpu.make_async_copy(src, dst, load_sem.at[k])
        load.start()
        loads.append(load)

    barrier = pltpu.get_barrier_semaphore()
    for dg in range(n_gr):
        for dt in range(n_tp):
            if dg or dt:
                pl.semaphore_signal(
                    barrier,
                    inc=1,
                    device_id=(lax.rem(g + dg, n_gr), f, lax.rem(t + dt, n_tp)),
                    device_id_type=MESH,
                )
    for near in (lax.rem(f + 1, n_fs), lax.rem(f + n_fs - 1, n_fs)):
        pl.semaphore_signal(barrier, inc=1, device_id=(g, near, t), device_id_type=MESH)

    def place(ref, origin):
        return ref.at[:, pl.ds(pl.multiple_of(origin * width, 128), width)]

    def round_matrix(n, m):
        place(outs[n][m], row)[...] = (gains[n] * gates_in[2 * n + m]).astype(jnp.bfloat16)

    def round_down(n):
        rounded = tall_in[n].astype(jnp.bfloat16)
        down_own[n] = rounded

        @pl.when(owner == t)
        def _():
            outs[n][2][slot, :, lanes(t * cols, cols)] = rounded

    def held(o):
        return jnp.logical_and(o >= first, o < first + per)

    def remote(src, dst, send, recv, to):
        return pltpu.make_async_remote_copy(
            src_ref=src,
            dst_ref=dst,
            send_sem=send,
            recv_sem=recv,
            device_id=to,
            device_id_type=MESH,
        )

    def spot(n, p, o, column):
        if p < 2:
            return place(outs[n][p], column * n_fs + o)
        if p < carried:
            at, size = crossed(column, p - 2)
        else:
            at, size = shared[p - carried]
        return outs[n][2].at[o - first, :, lanes(at, size)]

    def line(n, p, way, s):
        step = 1 if way == 0 else -1
        o = f - step * (s - 1)
        sems = line_send.at[n, p, way, s], line_recv.at[n, p, way, s]
        return remote(spot(n, p, o, g), spot(n, p, o, g), *sems, (g, f + step, t))

    def sends(p, way, s):
        step = 1 if way == 0 else -1
        o = f - step * (s - 1)
        fine = (f < n_fs - 1, o >= 0) if way == 0 else (f > 0, o <= n_fs - 1)
        ok = jnp.logical_and(*fine)
        return jnp.logical_and(ok, held(o)) if p >= 2 else ok

    def origin(way, s):
        return f - s if way == 0 else f + s

    def gets(p, way, s):
        o = origin(way, s)
        ok = o >= 0 if way == 0 else o <= n_fs - 1
        return jnp.logical_and(ok, held(o)) if p >= 2 else ok

    def ends(way):
        return f == n_fs - 1 if way == 0 else f == 0

    def landed(n, p, way, s):
        o = origin(way, s)
        sems = line_send.at[n, p, way, s], line_recv.at[n, p, way, s]
        return remote(spot(n, p, o, g), spot(n, p, o, g), *sems, (g, f, t))

    def pair(n, p, o):
        sems = pair_send.at[n, p, o], pair_recv.at[n, p, o]
        return remote(spot(n, p, o, g), spot(n, p, o, g), *sems, (1 - g, f, t))

    def pair_landed(n, p, o):
        sems = pair_send.at[n, p, o], pair_recv.at[n, p, o]
        return remote(spot(n, p, o, 1 - g), spot(n, p, o, 1 - g), *sems, (1 - g, f, t))

    def part(n, dg):
        return remote(
            down_own.at[n],
            outs[n][2].at[slot, :, lanes(t * cols, cols)],
            part_send.at[n, dg],
            part_recv.at[n, t],
            (lax.rem(g + dg, n_gr), f, owner),
        )

    def part_landed(n, src):
        return remote(
            down_own.at[n],
            outs[n][2].at[f - first, :, pl.ds(src * cols, cols)],
            part_send.at[n, 0],
            part_recv.at[n, src],
            (home, f, src),
        )

    def start_lines(n, p):
        for way in range(2):

            @pl.when(sends(p, way, 1))
            def _(way=way):
                line(n, p, way, 1).start()

    def give_part(n):
        @pl.when(owner != t)
        def _():
            part(n, 0).start()

    def start_down(n):
        @pl.when(held(f))
        def _():
            for src in range(n_tp):

                @pl.when(jnp.logical_or(home != g, t != src))
                def _(src=src):
                    part_landed(n, src).wait_recv()

        for p in range(2, count):
            start_lines(n, p)

    def forward(n, p, s):
        crosses, relays = p < carried, s < n_fs - 1
        for way in range(2):
            if not crosses and not relays:
                continue
            ready = gets(p, way, s)
            if not crosses:
                ready = jnp.logical_and(ready, jnp.logical_not(ends(way)))

            @pl.when(ready)
            def _(way=way):
                landed(n, p, way, s).wait_recv()
                if relays:

                    @pl.when(sends(p, way, s + 1))
                    def _():
                        line(n, p, way, s + 1).start()

                if crosses:
                    pair(n, p, origin(way, s)).start()

    def settle(n, p):
        for s in range(1, n_fs):
            for way in range(2):
                ready = gets(p, way, s)
                if s < n_fs - 1:
                    ready = jnp.logical_and(ready, ends(way))

                @pl.when(ready)
                def _(way=way, s=s):
                    landed(n, p, way, s).wait_recv()

    def pairs_in(n, p):
        for o in range(n_fs):
            if p < 2:
                pair_landed(n, p, o).wait_recv()
            else:

                @pl.when(jnp.logical_and(held(o), o != f))
                def _(o=o):
                    pair_landed(n, p, o).wait_recv()

    def drain(n):
        for p in range(carried):
            for o in range(n_fs):
                if p < 2:
                    pair(n, p, o).wait_send()
                else:

                    @pl.when(jnp.logical_and(held(o), o != f))
                    def _(p=p, o=o):
                        pair(n, p, o).wait_send()

        for p in range(count):
            for way in range(2):
                for s in range(1, n_fs):

                    @pl.when(sends(p, way, s))
                    def _(p=p, way=way, s=s):
                        line(n, p, way, s).wait_send()

        @pl.when(owner != t)
        def _():
            part(n, 0).wait_send()

        part(n, 1).wait_send()

    across = (((1,), (1,)), ((), ()))

    def unit(rows):
        return rows * lax.rsqrt(jnp.mean(rows * rows, axis=-1, keepdims=True) + 1e-06)

    def seat_of(j):
        return lax.rem(seat + 1 + j, pairs)

    def hide(n, source):
        @pl.loop(0, 2)
        def _(c):
            rows = jnp.concatenate([source[c, seat_of(j)] for j in range(pairs)], axis=0)
            gate = lax.dot_general(
                rows, outs[n][0][...], across, preferred_element_type=jnp.float32
            )
            upper = lax.dot_general(
                rows, outs[n][1][...], across, preferred_element_type=jnp.float32
            )
            hidden[c] = (jax.nn.silu(gate) * upper).astype(jnp.bfloat16)

    ranges = column_ranges(depth, g)
    steps = len(ranges)
    widths = [sum(size for _, size in part) for part in ranges]
    starts = [sum(widths[:k]) for k in range(steps)]
    spans = [pl.ds(starts[k], widths[k]) for k in range(steps)]
    kernel_groups = (range(steps), range(INSIDE))

    def mate(n, k):
        at = spans[k]
        return remote(
            mate_out.at[n, :, at],
            mate_in.at[n, :, at],
            mate_send.at[n, k],
            mate_recv.at[n, k],
            (g, f, t + 1 - 2 * core),
        )

    def share(n, k, j):
        at = spans[k]
        return remote(
            sums.at[n, j, :, at],
            sums_in.at[n, j, :, at],
            sum_send.at[n, k, j],
            sum_recv.at[n, k, j],
            (g, f, 2 * seat_of(j) + core),
        )

    def term(n, units, k):
        tiles = [
            jnp.dot(
                units,
                outs[n][2][:, :, lanes(at, size)].reshape(per * tall, size),
                preferred_element_type=jnp.float32,
            )
            for at, size in ranges[k]
        ]
        return tiles[0] if len(tiles) == 1 else jnp.concatenate(tiles, axis=1)

    def arrive(n, k):
        whole, pieces = groups[k - 1]
        for i in whole:
            settle(n, carried + i)
        for i in pieces:
            pairs_in(n, 2 + i)

    def offer(n, k):
        mate_out[n, :, spans[k]] = term(n, hidden[1 - core], k).astype(jnp.bfloat16)
        mate(n, k).start()

    def reduce(n, k):
        at = spans[k]
        mine = term(n, hidden[core], k)
        mate(n, k).wait_recv()
        both = mine + mate_in[n, :, at].astype(jnp.float32)
        if k in kernel_groups[n]:
            for j in range(pairs - 1):
                sums[n, j, :, at] = both[j * owned : (j + 1) * owned].astype(jnp.bfloat16)
                share(n, k, j).start()
            kept[:, at] = both[(pairs - 1) * owned :]
            return
        late = starts[k] - starts[INSIDE]
        for j in range(pairs - 1):
            late_sums[j, :, pl.ds(late, widths[k])] = both[j * owned : (j + 1) * owned].astype(
                jnp.bfloat16
            )
        passed = (pairs - 1) * owned
        done = 0
        for column, size in ranges[k]:
            late_rest[:, pl.ds(late + done, size)] = (
                stream[:, lanes(column, size)] + 0.5 * both[passed:, done : done + size]
            )
            done += size

    def collect(n, k, base, finish):
        for j in range(pairs - 1):
            share(n, k, j).wait_recv()
        total = kept[:, spans[k]]
        for j in range(pairs - 1):
            total += sums_in[n, j, :, spans[k]].astype(jnp.float32)
        passed = 0
        for at, size in ranges[k]:
            finish(lanes(at, size), base(lanes(at, size)) + 0.5 * total[:, passed : passed + size])
            passed += size

    def give(j):
        own = normed_all.at[core, seat]
        return remote(own, own, row_send.at[j], row_recv.at[j], (g, f, 2 * seat_of(j) + core))

    def given(j):
        src = lax.rem(seat - 1 - j + pairs, pairs)
        spot = normed_all.at[core, src]
        return remote(spot, spot, row_send.at[j], row_recv.at[j], (g, f, 2 * src + core))

    def pass_on(j):
        src = lax.rem(seat - 1 - j + 2 * pairs, pairs)
        spot = normed_all.at[core, src]
        at = pairs - 1 + (pairs - 1 if j < 0 else j)
        return remote(
            spot, spot, row_send.at[at], row_recv.at[at], (g, f, t + 1 - 2 * core)
        )

    def passed_on(j):
        src = lax.rem(seat - 1 - j + 2 * pairs, pairs)
        spot = normed_all.at[1 - core, src]
        at = pairs - 1 + (pairs - 1 if j < 0 else j)
        return remote(
            spot, spot, row_send.at[at], row_recv.at[at], (g, f, t + 1 - 2 * core)
        )

    loads[0].wait()
    loads[1].wait()
    round_matrix(0, 0)
    pl.semaphore_wait(barrier, n_gr * n_tp + 1)
    start_lines(0, 0)
    pair(0, 0, f).start()
    loads[2].wait()
    round_matrix(0, 1)
    start_lines(0, 1)
    pair(0, 1, f).start()
    loads[3].wait()
    round_down(0)
    part(0, 1).start()
    give_part(0)
    loads[5].wait()
    loads[6].wait()
    round_down(1)
    give_part(1)
    loads[7].wait()
    round_matrix(1, 0)
    loads[8].wait()
    round_matrix(1, 1)
    loads[4].wait()

    @pl.loop(0, n_tp)
    def _(i):
        normed[lax.rem(i, 2), i // 2] = unit(prompt[i].astype(jnp.float32)).astype(jnp.bfloat16)

    def first_half(n):
        for m in range(2):
            forward(n, m, 1)

    def second_half(n):
        for s in range(2, n_fs):
            for m in range(2):
                forward(n, m, s)
            if s == 2:
                start_down(n)

    def downs(n):
        for p in range(2, carried):
            for s in range(1, n_fs):
                forward(n, p, s)
        for p in range(carried, count):
            for s in range(1, n_fs):
                forward(n, p, s)

    first_half(0)
    second_half(0)
    downs(0)
    part(1, 1).start()
    for m in range(2):
        start_lines(1, m)
        pair(1, m, f).start()
    for m in range(2):
        pairs_in(0, m)
    hide(0, normed)
    offer(0, 0)
    for k in range(1, steps):
        arrive(0, k)
        offer(0, k)
        reduce(0, k - 1)
    reduce(0, steps - 1)
    first_half(1)

    def own_prompt(at):
        return prompt[t, :, at].astype(jnp.float32)

    def keep_stream(at, value):
        stream[:, at] = value

    for k in range(steps):
        collect(0, k, own_prompt, keep_stream)
    normed_all[core, seat] = unit(stream[...]).astype(jnp.bfloat16)
    for j in range(pairs - 1):
        give(j).start()
    pass_on(-1).start()
    for s in range(2, n_fs):
        for m in range(2):
            forward(1, m, s)
        if s == 2:
            start_down(1)
            for j in range(pairs - 1):
                given(j).wait_recv()
                pass_on(j).start()
    downs(1)
    for j in range(-1, pairs - 1):
        passed_on(j).wait_recv()
    for m in range(2):
        pairs_in(1, m)
    hide(1, normed_all)

    def keep_mixed(at, value):
        mixed_ref[:, at] = value.astype(jnp.bfloat16)

    def own_stream(at):
        return stream[:, at]

    offer(1, 0)
    arrive(1, 1)
    offer(1, 1)
    reduce(1, 0)
    reduce(1, 1)
    for k in range(2, steps):
        arrive(1, k)
        offer(1, k)
        reduce(1, k)
    drain(0)
    drain(1)
    for k in kernel_groups[1]:
        collect(1, k, own_stream, keep_mixed)
    for j in range(pairs - 1):
        give(j).wait_send()
    for j in range(-1, pairs - 1):
        pass_on(j).wait_send()
    for n in range(2):
        for k in range(steps):
            mate(n, k).wait_send()
            if k in kernel_groups[n]:
                for j in range(pairs - 1):
                    share(n, k, j).wait_send()


def write_kernel(*refs):
    count = (len(refs) - 1) // 2
    sems = refs[-1]
    copies = [
        pltpu.make_async_copy(refs[k], refs[count + k], sems.at[k]) for k in range(count)
    ]
    for copy in copies:
        copy.start()
    for copy in copies:
        copy.wait()


def written(arrays):
    arrays = [pltpu.with_memory_space_constraint(a, pltpu.VMEM) for a in arrays]
    return pl.pallas_call(
        write_kernel,
        out_shape=tuple(jax.ShapeDtypeStruct(a.shape, a.dtype) for a in arrays),
        in_specs=[pl.BlockSpec(memory_space=pltpu.VMEM)] * len(arrays),
        out_specs=(pl.BlockSpec(memory_space=pl.ANY),) * len(arrays),
        scratch_shapes=[pltpu.SemaphoreType.DMA((len(arrays),))],
        compiler_params=pltpu.CompilerParams(vmem_limit_bytes=2**20),
        cost_estimate=pl.CostEstimate(
            flops=2 * 10**9, bytes_accessed=32 * 2**20, transcendentals=0
        ),
    )(*arrays)


def finish_kernel(early_ref, rest_ref, *refs):
    mixed_ref = refs[-1]
    depth = early_ref.shape[1]
    total = rest_ref[...]
    for received in refs[:-1]:
        total += 0.5 * received[...].astype(jnp.float32)
    total = total.astype(mixed_ref.dtype)
    ranges = column_ranges(depth, lax.axis_index("gr"))
    done = 0
    for k, columns in enumerate(ranges):
        for at, size in columns:
            at = pl.ds(pl.multiple_of(at, 128), size)
            if k < INSIDE:
                mixed_ref[:, at] = early_ref[:, at]
            else:
                mixed_ref[:, at] = total[:, done : done + size]
                done += size


def finished(early, rest, received):
    return pl.pallas_call(
        finish_kernel,
        out_shape=jax.ShapeDtypeStruct(early.shape, early.dtype),
        compiler_params=pltpu.CompilerParams(vmem_limit_bytes=4 * 2**20),
    )(early, rest, *received)


def fused(sizes, prompt, *weights):
    n_gr, n_fs, n_tp = sizes
    per = n_gr * n_fs // n_tp
    tokens, depth = prompt.shape
    owned = tokens // n_tp
    rows, width = weights[1].shape
    tall, cols = weights[3].shape
    pairs = n_tp // 2
    split, shared, groups = down_pieces(depth)
    steps, pieces = 1 + len(groups), 2 + len(split) + len(shared)
    late = sum(size for columns in column_ranges(depth, 0)[INSIDE:] for _, size in columns)
    vmem = pl.BlockSpec(memory_space=pltpu.VMEM)
    hbm = pl.BlockSpec(memory_space=pltpu.HBM)
    dma = pltpu.SemaphoreType.DMA
    across = pltpu.VMEM((width, n_gr * n_fs * rows), jnp.bfloat16)
    down = pltpu.VMEM((per, tall, n_tp * cols), jnp.bfloat16)
    operands = [prompt.reshape(n_tp, owned, depth)]
    for n in range(2):
        gain, gate, up, tall_block = weights[4 * n : 4 * n + 4]
        operands += [gain[None, :], gate.T, up.T, tall_block]
    results = pl.pallas_call(
        functools.partial(fused_kernel, n_gr, n_fs, n_tp),
        out_shape=(across, across, down) * 2
        + (
            pltpu.VMEM((owned, depth), jnp.bfloat16),
            pltpu.VMEM((pairs - 1, owned, late), jnp.bfloat16),
            pltpu.VMEM((owned, late), jnp.float32),
        ),
        in_specs=[hbm] * 9,
        out_specs=(vmem,) * 9,
        scratch_shapes=[
            pltpu.VMEM((n_tp, owned, depth), prompt.dtype),
            pltpu.VMEM((2, 1, rows), jnp.float32),
            pltpu.VMEM((2, tall, cols), jnp.float32),
            pltpu.VMEM((4, width, rows), jnp.float32),
            dma((9,)),
            pltpu.VMEM((2, tall, cols), jnp.bfloat16),
            pltpu.VMEM((2, pairs, owned, depth), jnp.bfloat16),
            pltpu.VMEM((2, pairs, owned, depth), jnp.bfloat16),
            pltpu.VMEM((2, pairs * owned, width), jnp.bfloat16),
            pltpu.VMEM((2, pairs * owned, depth), jnp.bfloat16),
            pltpu.VMEM((2, pairs * owned, depth), jnp.bfloat16),
            pltpu.VMEM((2, pairs - 1, owned, depth), jnp.bfloat16),
            pltpu.VMEM((2, pairs - 1, owned, depth), jnp.bfloat16),
            pltpu.VMEM((owned, depth), jnp.float32),
            pltpu.VMEM((owned, depth), jnp.float32),
            dma((2, pieces, 2, n_fs)),
            dma((2, pieces, 2, n_fs)),
            dma((2, 2 + len(split), n_fs)),
            dma((2, 2 + len(split), n_fs)),
            dma((2, n_gr)),
            dma((2, n_tp)),
            dma((2, steps)),
            dma((2, steps)),
            dma((2, steps, pairs - 1)),
            dma((2, steps, pairs - 1)),
            dma((2 * pairs - 1,)),
            dma((2 * pairs - 1,)),
        ],
        compiler_params=pltpu.CompilerParams(
            collective_id=2, has_side_effects=True, vmem_limit_bytes=44 * 2**20
        ),
    )(*operands)
    *served, early, sums, rest = results
    received = [
        lax.ppermute(
            sums[j], "tp", [(t, (t + 2 * (1 + j)) % n_tp) for t in range(n_tp)]
        )
        for j in range(pairs - 1)
    ]
    gate_a, up_a, down_a, gate_b, up_b, down_b = written(served)
    mixed = finished(early, rest, received)

    def flat(a):
        return a.reshape(per * tall, n_tp * cols)

    return (gate_a.T, up_a.T, flat(down_a), gate_b.T, up_b.T, flat(down_b), mixed)


def normalize(rows):
    rows = rows.astype(jnp.float32)
    scale = lax.rsqrt(jnp.mean(rows * rows, axis=-1, keepdims=True) + 1e-06)
    return (rows * scale).astype(jnp.bfloat16)


def hidden_units(normed, w_gate, w_up):
    gate = jnp.dot(normed, w_gate, preferred_element_type=jnp.float32)
    upper = jnp.dot(normed, w_up, preferred_element_type=jnp.float32)
    return (jax.nn.silu(gate) * upper).astype(jnp.bfloat16)


def rounded_term(hidden, w_down):
    return jnp.dot(hidden, w_down, preferred_element_type=jnp.float32).astype(jnp.bfloat16)


def suits(sizes, prompt, gate, down):
    n_gr, n_fs, n_tp = sizes
    per = n_gr * n_fs // n_tp
    return (
        n_gr == 2
        and n_tp % 2 == 0
        and per > 0
        and per * n_tp == n_gr * n_fs
        and n_fs % per == 0
        and gate.shape[0] % 128 == 0
        and down.shape[0] % 16 == 0
        and down.shape[1] % 128 == 0
        and prompt.shape[1] % 2048 == 0
        and prompt.shape[0] % (16 * n_tp) == 0
    )


def shards(
    sizes,
    prompt,
    gain_first,
    gate_first,
    up_first,
    down_first,
    gain_second,
    gate_second,
    up_second,
    down_second,
):
    if suits(sizes, prompt, gate_first, down_first):
        return fused(
            sizes,
            prompt,
            gain_first,
            gate_first,
            up_first,
            down_first,
            gain_second,
            gate_second,
            up_second,
            down_second,
        )
    gate_a, up_a, down_a = gather(sizes, 0, gain_first, gate_first, up_first, down_first)
    hidden_a = hidden_units(normalize(prompt), gate_a, up_a)
    term_a = rounded_term(hidden_a, down_a)
    term_a, gain_second = lax.optimization_barrier((term_a, gain_second))
    branch_a = lax.psum(term_a, "tp").astype(jnp.float32)
    gate_b, up_b, down_b = gather(sizes, 1, gain_second, gate_second, up_second, down_second)
    stream = prompt.astype(jnp.float32) + 0.5 * branch_a
    hidden_b = hidden_units(normalize(stream), gate_b, up_b)
    owned = hidden_b.shape[0] // lax.axis_size("tp")
    branch_b = lax.psum_scatter(
        rounded_term(hidden_b, down_b), "tp", scatter_dimension=0, tiled=True
    ).astype(jnp.float32)
    own_stream = lax.dynamic_slice_in_dim(stream, lax.axis_index("tp") * owned, owned, 0)
    mixed = (own_stream + 0.5 * branch_b).astype(jnp.bfloat16)
    return (gate_a, up_a, down_a, gate_b, up_b, down_b, mixed)


def solution(mesh):
    sizes = (mesh.shape["gr"], mesh.shape["fs"], mesh.shape["tp"])
    return jax.shard_map(
        functools.partial(shards, sizes),
        mesh=mesh,
        in_specs=(
            P(("gr", "fs"), None),
            P(("gr", "fs")),
            P(("gr", "fs"), "tp"),
            P(("gr", "fs"), "tp"),
            P(("gr", "fs"), "tp"),
            P(("gr", "fs")),
            P(("gr", "fs"), "tp"),
            P(("gr", "fs"), "tp"),
            P(("gr", "fs"), "tp"),
        ),
        out_specs=(
            P(None, "tp"),
            P(None, "tp"),
            P("tp", None),
            P(None, "tp"),
            P(None, "tp"),
            P("tp", None),
            P(("gr", "fs", "tp"), None),
        ),
        check_vma=False,
    )
```

```python
import functools

import jax
import jax.numpy as jnp
from jax import lax
from jax.experimental import pallas as pl
from jax.experimental.pallas import tpu as pltpu
from jax.sharding import PartitionSpec as P

MESH = pl.DeviceIdType.MESH


def gather_kernel(
    n_gr,
    n_fs,
    n_tp,
    gain_ref,
    gate_ref,
    up_ref,
    down_ref,
    gate_out,
    up_out,
    down_out,
    down_own,
    line_send,
    line_recv,
    pair_send,
    pair_recv,
    part_send,
    part_recv,
):
    g, f, t = lax.axis_index("gr"), lax.axis_index("fs"), lax.axis_index("tp")
    per = n_gr * n_fs // n_tp
    cols = down_ref.shape[1]
    first = lax.rem(t * per, n_fs)
    home = (t * per) // n_fs
    row = g * n_fs + f
    owner = row // per
    slot = lax.rem(row, per)

    width = gate_ref.shape[1]

    def place(ref, origin):
        if len(ref.shape) == 3:
            return ref.at[origin]
        return ref.at[:, pl.ds(pl.multiple_of(origin * width, 128), width)]

    gain = gain_ref[...]
    place(gate_out, row)[...] = (gain * gate_ref[...]).astype(jnp.bfloat16)
    place(up_out, row)[...] = (gain * up_ref[...]).astype(jnp.bfloat16)
    down_own[...] = down_ref[...].astype(jnp.bfloat16)

    @pl.when(owner == t)
    def _():
        down_out[slot, :, pl.ds(pl.multiple_of(t * cols, 128), cols)] = down_ref[...].astype(
            jnp.bfloat16
        )

    barrier = pltpu.get_barrier_semaphore()
    for dg in range(n_gr):
        for dt in range(n_tp):
            if dg or dt:
                pl.semaphore_signal(
                    barrier,
                    inc=1,
                    device_id=(lax.rem(g + dg, n_gr), f, lax.rem(t + dt, n_tp)),
                    device_id_type=MESH,
                )

    for near in (lax.rem(f + 1, n_fs), lax.rem(f + n_fs - 1, n_fs)):
        pl.semaphore_signal(barrier, inc=1, device_id=(g, near, t), device_id_type=MESH)
    pl.semaphore_wait(barrier, n_gr * n_tp + 1)

    outs = (gate_out, up_out)

    def held(o):
        return jnp.logical_and(o >= first, o < first + per)

    def block(m, o):
        if m < 2:
            return place(outs[m], g * n_fs + o)
        return down_out.at[o - first]

    def line(m, way, s):
        step = 1 if way == 0 else -1
        o = f - step * (s - 1)
        return pltpu.make_async_remote_copy(
            src_ref=block(m, o),
            dst_ref=block(m, o),
            send_sem=line_send.at[m, way, s],
            recv_sem=line_recv.at[m, way, s],
            device_id=(g, f + step, t),
            device_id_type=MESH,
        )

    def sends(m, way, s):
        step = 1 if way == 0 else -1
        o = f - step * (s - 1)
        fine = (f < n_fs - 1, o >= 0) if way == 0 else (f > 0, o <= n_fs - 1)
        ok = jnp.logical_and(*fine)
        return jnp.logical_and(ok, held(o)) if m == 2 else ok

    def gets(m, way, s):
        o = f - s if way == 0 else f + s
        ok = o >= 0 if way == 0 else o <= n_fs - 1
        return jnp.logical_and(ok, held(o)) if m == 2 else ok

    def landed(m, way, s):
        o = f - s if way == 0 else f + s
        return pltpu.make_async_remote_copy(
            src_ref=block(m, o),
            dst_ref=block(m, o),
            send_sem=line_send.at[m, way, s],
            recv_sem=line_recv.at[m, way, s],
            device_id=(g, f, t),
            device_id_type=MESH,
        )

    def pair(m, dg, o):
        return pltpu.make_async_remote_copy(
            src_ref=place(outs[m], g * n_fs + o),
            dst_ref=place(outs[m], g * n_fs + o),
            send_sem=pair_send.at[m, dg, o],
            recv_sem=pair_recv.at[m, dg, o],
            device_id=(lax.rem(g + dg, n_gr), f, t),
            device_id_type=MESH,
        )

    def pair_landed(m, dg, o):
        src = lax.rem(g - dg + n_gr, n_gr)
        return pltpu.make_async_remote_copy(
            src_ref=place(outs[m], src * n_fs + o),
            dst_ref=place(outs[m], src * n_fs + o),
            send_sem=pair_send.at[m, dg, o],
            recv_sem=pair_recv.at[m, dg, o],
            device_id=(src, f, t),
            device_id_type=MESH,
        )

    def part(dg):
        to = lax.rem(g + dg, n_gr)
        return pltpu.make_async_remote_copy(
            src_ref=down_own,
            dst_ref=down_out.at[slot, :, pl.ds(pl.multiple_of(t * cols, 128), cols)],
            send_sem=part_send.at[dg],
            recv_sem=part_recv.at[t],
            device_id=(to, f, owner),
            device_id_type=MESH,
        )

    def part_landed(src):
        return pltpu.make_async_remote_copy(
            src_ref=down_own,
            dst_ref=down_out.at[f - first, :, pl.ds(src * cols, cols)],
            send_sem=part_send.at[0],
            recv_sem=part_recv.at[src],
            device_id=(home, f, src),
            device_id_type=MESH,
        )

    for m in range(2):
        for way in range(2):

            @pl.when(sends(m, way, 1))
            def _(m=m, way=way):
                line(m, way, 1).start()

        for dg in range(1, n_gr):
            pair(m, dg, f).start()
    for dg in range(n_gr):
        if dg == 0:

            @pl.when(owner != t)
            def _():
                part(0).start()

        else:
            part(dg).start()

    @pl.when(held(f))
    def _():
        for src in range(n_tp):

            @pl.when(jnp.logical_or(home != g, t != src))
            def _(src=src):
                part_landed(src).wait_recv()

    for way in range(2):

        @pl.when(sends(2, way, 1))
        def _(way=way):
            line(2, way, 1).start()

    for s in range(1, n_fs):
        for m in range(3):
            for way in range(2):

                @pl.when(gets(m, way, s))
                def _(m=m, way=way, s=s):
                    landed(m, way, s).wait_recv()
                    if s < n_fs - 1:

                        @pl.when(sends(m, way, s + 1))
                        def _():
                            line(m, way, s + 1).start()

                    if m < 2:
                        o = f - s if way == 0 else f + s
                        for dg in range(1, n_gr):
                            pair(m, dg, o).start()

    for m in range(2):
        for dg in range(1, n_gr):
            for o in range(n_fs):
                pair_landed(m, dg, o).wait_recv()
                pair(m, dg, o).wait_send()
    for m in range(3):
        for way in range(2):
            for s in range(1, n_fs):

                @pl.when(sends(m, way, s))
                def _(m=m, way=way, s=s):
                    line(m, way, s).wait_send()

    for dg in range(n_gr):
        if dg == 0:

            @pl.when(owner != t)
            def _():
                part(0).wait_send()

        else:
            part(dg).wait_send()


def gather(sizes, call, gain, gate, up, down):
    n_gr, n_fs, n_tp = sizes
    per = n_gr * n_fs // n_tp
    rows, width = gate.shape
    wide = rows % 128 == 0
    whole = (width, n_gr * n_fs * rows) if wide else (n_gr * n_fs, width, rows)
    tall, cols = down.shape
    vmem = pl.BlockSpec(memory_space=pltpu.VMEM)
    dma = pltpu.SemaphoreType.DMA
    gate_all, up_all, down_all = pl.pallas_call(
        functools.partial(gather_kernel, n_gr, n_fs, n_tp),
        out_shape=(
            jax.ShapeDtypeStruct(whole, jnp.bfloat16),
            jax.ShapeDtypeStruct(whole, jnp.bfloat16),
            jax.ShapeDtypeStruct((per, tall, n_tp * cols), jnp.bfloat16),
        ),
        in_specs=[vmem] * 4,
        out_specs=(vmem,) * 3,
        scratch_shapes=[
            pltpu.VMEM((tall, cols), jnp.bfloat16),
            dma((3, 2, n_fs)),
            dma((3, 2, n_fs)),
            dma((2, n_gr, n_fs)),
            dma((2, n_gr, n_fs)),
            dma((n_gr,)),
            dma((n_tp,)),
        ],
        compiler_params=pltpu.CompilerParams(
            collective_id=call, has_side_effects=True, vmem_limit_bytes=32 * 2**20
        ),
        cost_estimate=pl.CostEstimate(
            flops=10**10, bytes_accessed=16 * 2**20, transcendentals=0
        ),
    )(gain[None, :], gate.T, up.T, down)

    def upright(a):
        return a.T if wide else a.transpose(0, 2, 1).reshape(n_gr * n_fs * rows, width)

    return (
        upright(gate_all),
        upright(up_all),
        down_all.reshape(per * tall, n_tp * cols),
    )


SPLIT = ((3,), (3, 1, 1))
SHARED = ((5, 5), (3, 2, 1))
GROUPS = (
    (((0,), ()), ((1,), (0,))),
    (((0,), ()), ((1,), (0,)), ((2,), (1, 2))),
)


def laid(start, sizes):
    return tuple((start + sum(sizes[:i]), size) for i, size in enumerate(sizes))


def down_pieces(n, depth, column):
    unit = depth // 16
    split = [unit * size for size in SPLIT[n]]
    shared = [unit * size for size in SHARED[n]]
    return laid(sum(shared) + column * sum(split), split), laid(0, shared)


def column_ranges(n, depth, g):
    own, shared = down_pieces(n, depth, g)
    other, _ = down_pieces(n, depth, 1 - g)
    ranges = [((own[0][0], sum(size for _, size in own)),)]
    for whole, pieces in GROUPS[n]:
        ranges.append(tuple(shared[i] for i in whole) + tuple(other[i] for i in pieces))
    return ranges


INSIDE = 2


def fused_kernel(
    n_gr,
    n_fs,
    n_tp,
    prompt_in,
    gain_in_a,
    gate_in_a,
    up_in_a,
    down_in_a,
    gain_in_b,
    gate_in_b,
    up_in_b,
    down_in_b,
    gate_out_a,
    up_out_a,
    down_out_a,
    gate_out_b,
    up_out_b,
    down_out_b,
    mixed_ref,
    late_sums,
    late_rest,
    prompt,
    gains,
    tall_in,
    gates_in,
    load_sem,
    down_own,
    normed,
    normed_all,
    hidden,
    mate_out,
    mate_in,
    sums,
    sums_in,
    kept,
    stream,
    line_send,
    line_recv,
    pair_send,
    pair_recv,
    part_send,
    part_recv,
    mate_send,
    mate_recv,
    sum_send,
    sum_recv,
    row_send,
    row_recv,
):
    g, f, t = lax.axis_index("gr"), lax.axis_index("fs"), lax.axis_index("tp")
    per = n_gr * n_fs // n_tp
    tall, cols = down_in_a.shape
    width = gate_in_a.shape[1]
    owned, depth = prompt.shape[1], prompt.shape[2]
    first = lax.rem(t * per, n_fs)
    home = (t * per) // n_fs
    row = g * n_fs + f
    owner = row // per
    slot = lax.rem(row, per)
    pairs = n_tp // 2
    seat, core = t // 2, lax.rem(t, 2)
    outs = ((gate_out_a, up_out_a, down_out_a), (gate_out_b, up_out_b, down_out_b))

    carried = [2 + len(split) for split in SPLIT]
    count = [c + len(shared) for c, shared in zip(carried, SHARED)]

    def lanes(at, size):
        return pl.ds(pl.multiple_of(at, 128), size)

    loads = []
    for k, (src, dst) in enumerate(
        (
            (gain_in_a, gains.at[0]),
            (gate_in_a, gates_in.at[0]),
            (up_in_a, gates_in.at[1]),
            (down_in_a, tall_in.at[0]),
            (prompt_in, prompt),
            (gain_in_b, gains.at[1]),
            (down_in_b, tall_in.at[1]),
            (gate_in_b, gates_in.at[2]),
            (up_in_b, gates_in.at[3]),
        )
    ):
        load = pltpu.make_async_copy(src, dst, load_sem.at[k])
        load.start()
        loads.append(load)

    barrier = pltpu.get_barrier_semaphore()
    for dg in range(n_gr):
        for dt in range(n_tp):
            if dg or dt:
                pl.semaphore_signal(
                    barrier,
                    inc=1,
                    device_id=(lax.rem(g + dg, n_gr), f, lax.rem(t + dt, n_tp)),
                    device_id_type=MESH,
                )
    for near in (lax.rem(f + 1, n_fs), lax.rem(f + n_fs - 1, n_fs)):
        pl.semaphore_signal(barrier, inc=1, device_id=(g, near, t), device_id_type=MESH)

    def place(ref, origin):
        return ref.at[:, pl.ds(pl.multiple_of(origin * width, 128), width)]

    def round_matrix(n, m):
        place(outs[n][m], row)[...] = (gains[n] * gates_in[2 * n + m]).astype(jnp.bfloat16)

    def round_down(n):
        rounded = tall_in[n].astype(jnp.bfloat16)
        down_own[n] = rounded

        @pl.when(owner == t)
        def _():
            outs[n][2][slot, :, lanes(t * cols, cols)] = rounded

    def held(o):
        return jnp.logical_and(o >= first, o < first + per)

    def remote(src, dst, send, recv, to):
        return pltpu.make_async_remote_copy(
            src_ref=src,
            dst_ref=dst,
            send_sem=send,
            recv_sem=recv,
            device_id=to,
            device_id_type=MESH,
        )

    def spot(n, p, o, column):
        if p < 2:
            return place(outs[n][p], column * n_fs + o)
        split, shared = down_pieces(n, depth, column)
        at, size = (split + shared)[p - 2]
        return outs[n][2].at[o - first, :, lanes(at, size)]

    def seat_in(n, p, o, most):
        blocks, downs_before = 2 * n + p, n * (count[0] - 2) + p - 2
        if p < 2:
            return blocks * (n_fs + most) + o
        return 4 * (n_fs + most) + downs_before * (per + most) + o - first

    def line_sems(n, p, way, s, o):
        own = (n_fs if p < 2 else per + first) if s == 1 and way == 1 else o
        return line_send.at[seat_in(n, p, own, 1)], line_recv.at[seat_in(n, p, o, 0)]

    def line(n, p, way, s):
        step = 1 if way == 0 else -1
        o = f - step * (s - 1)
        sems = line_sems(n, p, way, s, o)
        return remote(spot(n, p, o, g), spot(n, p, o, g), *sems, (g, f + step, t))

    def sends(p, way, s):
        step = 1 if way == 0 else -1
        o = f - step * (s - 1)
        fine = (f < n_fs - 1, o >= 0) if way == 0 else (f > 0, o <= n_fs - 1)
        ok = jnp.logical_and(*fine)
        return jnp.logical_and(ok, held(o)) if p >= 2 else ok

    def origin(way, s):
        return f - s if way == 0 else f + s

    def gets(p, way, s):
        o = origin(way, s)
        ok = o >= 0 if way == 0 else o <= n_fs - 1
        return jnp.logical_and(ok, held(o)) if p >= 2 else ok

    def ends(way):
        return f == n_fs - 1 if way == 0 else f == 0

    def landed(n, p, way, s):
        o = origin(way, s)
        sems = line_sems(n, p, 0, s, o)
        return remote(spot(n, p, o, g), spot(n, p, o, g), *sems, (g, f, t))

    def pair_seat(n, p, o):
        if p < 2:
            return (2 * n + p) * n_fs + o
        return 4 * n_fs + (n * (carried[0] - 2) + p - 2) * per + o - first

    def pair(n, p, o):
        sems = pair_send.at[pair_seat(n, p, o)], pair_recv.at[pair_seat(n, p, o)]
        return remote(spot(n, p, o, g), spot(n, p, o, g), *sems, (1 - g, f, t))

    def pair_landed(n, p, o):
        sems = pair_send.at[pair_seat(n, p, o)], pair_recv.at[pair_seat(n, p, o)]
        return remote(spot(n, p, o, 1 - g), spot(n, p, o, 1 - g), *sems, (1 - g, f, t))

    def part(n, dg):
        return remote(
            down_own.at[n],
            outs[n][2].at[slot, :, lanes(t * cols, cols)],
            part_send.at[n, dg],
            part_recv.at[n, t],
            (lax.rem(g + dg, n_gr), f, owner),
        )

    def part_landed(n, src):
        return remote(
            down_own.at[n],
            outs[n][2].at[f - first, :, pl.ds(src * cols, cols)],
            part_send.at[n, 0],
            part_recv.at[n, src],
            (home, f, src),
        )

    def start_lines(n, p):
        for way in range(2):

            @pl.when(sends(p, way, 1))
            def _(way=way):
                line(n, p, way, 1).start()

    def give_part(n):
        @pl.when(owner != t)
        def _():
            part(n, 0).start()

    def parts_in(n):
        @pl.when(held(f))
        def _():
            for src in range(n_tp):

                @pl.when(jnp.logical_or(home != g, t != src))
                def _(src=src):
                    part_landed(n, src).wait_recv()

    def forward(n, p, s):
        crosses, relays = p < carried[n], s < n_fs - 1
        for way in range(2):
            if not crosses and not relays:
                continue
            ready = gets(p, way, s)
            if not crosses:
                ready = jnp.logical_and(ready, jnp.logical_not(ends(way)))

            @pl.when(ready)
            def _(way=way):
                landed(n, p, way, s).wait_recv()
                if relays:

                    @pl.when(sends(p, way, s + 1))
                    def _():
                        line(n, p, way, s + 1).start()

                if crosses:
                    pair(n, p, origin(way, s)).start()

    def settle(n, p):
        for s in range(1, n_fs):
            for way in range(2):
                ready = gets(p, way, s)
                if s < n_fs - 1:
                    ready = jnp.logical_and(ready, ends(way))

                @pl.when(ready)
                def _(way=way, s=s):
                    landed(n, p, way, s).wait_recv()

    def pairs_in(n, p):
        for o in range(n_fs):
            if p < 2:
                pair_landed(n, p, o).wait_recv()
            else:

                @pl.when(jnp.logical_and(held(o), o != f))
                def _(o=o):
                    pair_landed(n, p, o).wait_recv()

    def drain(n):
        for p in range(carried[n]):
            for o in range(n_fs):
                if p < 2:
                    pair(n, p, o).wait_send()
                else:

                    @pl.when(jnp.logical_and(held(o), o != f))
                    def _(p=p, o=o):
                        pair(n, p, o).wait_send()

        for p in range(count[n]):
            for way in range(2):
                for s in range(1, n_fs):

                    @pl.when(sends(p, way, s))
                    def _(p=p, way=way, s=s):
                        line(n, p, way, s).wait_send()

        @pl.when(owner != t)
        def _():
            part(n, 0).wait_send()

        part(n, 1).wait_send()

    across = (((1,), (1,)), ((), ()))

    def unit(rows):
        return rows * lax.rsqrt(jnp.mean(rows * rows, axis=-1, keepdims=True) + 1e-06)

    def seat_of(j):
        return lax.rem(seat + 1 + j, pairs)

    def hide(n, source):
        @pl.loop(0, 2)
        def _(c):
            rows = jnp.concatenate([source[c, seat_of(j)] for j in range(pairs)], axis=0)
            gate = lax.dot_general(
                rows, outs[n][0][...], across, preferred_element_type=jnp.float32
            )
            upper = lax.dot_general(
                rows, outs[n][1][...], across, preferred_element_type=jnp.float32
            )
            hidden[c] = (jax.nn.silu(gate) * upper).astype(jnp.bfloat16)

    ranges = [column_ranges(n, depth, g) for n in range(2)]
    steps = [len(part) for part in ranges]
    widths = [[sum(size for _, size in columns) for columns in part] for part in ranges]
    starts = [[sum(sizes[:k]) for k in range(len(sizes))] for sizes in widths]
    spans = [[pl.ds(*at) for at in zip(starts[n], widths[n])] for n in range(2)]
    kernel_groups = (range(steps[0]), range(INSIDE))

    def mate(n, k):
        at = spans[n][k]
        return remote(
            mate_out.at[n, :, at],
            mate_in.at[n, :, at],
            mate_send.at[n, k],
            mate_recv.at[n, k],
            (g, f, t + 1 - 2 * core),
        )

    def share(n, k, j):
        at = spans[n][k]
        return remote(
            sums.at[n, j, :, at],
            sums_in.at[n, j, :, at],
            sum_send.at[n, k, j],
            sum_recv.at[n, k, j],
            (g, f, 2 * seat_of(j) + core),
        )

    def term(n, units, k):
        tiles = [
            jnp.dot(
                units,
                outs[n][2][:, :, lanes(at, size)].reshape(per * tall, size),
                preferred_element_type=jnp.float32,
            )
            for at, size in ranges[n][k]
        ]
        return tiles[0] if len(tiles) == 1 else jnp.concatenate(tiles, axis=1)

    def arrive(n, k):
        whole, pieces = GROUPS[n][k - 1]
        for i in whole:
            settle(n, carried[n] + i)
        for i in pieces:
            pairs_in(n, 2 + i)

    def offer(n, k):
        mate_out[n, :, spans[n][k]] = term(n, hidden[1 - core], k).astype(jnp.bfloat16)
        mate(n, k).start()

    def reduce(n, k):
        at = spans[n][k]
        mine = term(n, hidden[core], k)
        mate(n, k).wait_recv()
        both = mine + mate_in[n, :, at].astype(jnp.float32)
        if k in kernel_groups[n]:
            for j in range(pairs - 1):
                sums[n, j, :, at] = both[j * owned : (j + 1) * owned].astype(jnp.bfloat16)
                share(n, k, j).start()
            kept[:, at] = both[(pairs - 1) * owned :]
            return
        late = starts[n][k] - starts[n][INSIDE]
        for j in range(pairs - 1):
            late_sums[j, :, pl.ds(late, widths[n][k])] = both[j * owned : (j + 1) * owned].astype(
                jnp.bfloat16
            )
        passed = (pairs - 1) * owned
        done = 0
        for column, size in ranges[n][k]:
            late_rest[:, pl.ds(late + done, size)] = (
                stream[:, lanes(column, size)] + 0.5 * both[passed:, done : done + size]
            )
            done += size

    def collect(n, k, base, finish):
        for j in range(pairs - 1):
            share(n, k, j).wait_recv()
        total = kept[:, spans[n][k]]
        for j in range(pairs - 1):
            total += sums_in[n, j, :, spans[n][k]].astype(jnp.float32)
        passed = 0
        for at, size in ranges[n][k]:
            finish(lanes(at, size), base(lanes(at, size)) + 0.5 * total[:, passed : passed + size])
            passed += size

    def give(j):
        own = normed_all.at[core, seat]
        return remote(own, own, row_send.at[j], row_recv.at[j], (g, f, 2 * seat_of(j) + core))

    def given(j):
        src = lax.rem(seat - 1 - j + pairs, pairs)
        spot = normed_all.at[core, src]
        return remote(spot, spot, row_send.at[j], row_recv.at[j], (g, f, 2 * src + core))

    def pass_on(j):
        src = lax.rem(seat - 1 - j + 2 * pairs, pairs)
        spot = normed_all.at[core, src]
        at = pairs - 1 + (pairs - 1 if j < 0 else j)
        return remote(
            spot, spot, row_send.at[at], row_recv.at[at], (g, f, t + 1 - 2 * core)
        )

    def passed_on(j):
        src = lax.rem(seat - 1 - j + 2 * pairs, pairs)
        spot = normed_all.at[1 - core, src]
        at = pairs - 1 + (pairs - 1 if j < 0 else j)
        return remote(
            spot, spot, row_send.at[at], row_recv.at[at], (g, f, t + 1 - 2 * core)
        )

    loads[0].wait()
    loads[1].wait()
    round_matrix(0, 0)
    pl.semaphore_wait(barrier, n_gr * n_tp + 1)
    start_lines(0, 0)
    pair(0, 0, f).start()
    loads[2].wait()
    round_matrix(0, 1)
    start_lines(0, 1)
    pair(0, 1, f).start()
    loads[3].wait()
    round_down(0)
    part(0, 1).start()
    give_part(0)
    loads[5].wait()
    loads[6].wait()
    round_down(1)
    give_part(1)
    loads[7].wait()
    round_matrix(1, 0)
    loads[8].wait()
    round_matrix(1, 1)
    loads[4].wait()

    @pl.loop(0, n_tp)
    def _(i):
        normed[lax.rem(i, 2), i // 2] = unit(prompt[i].astype(jnp.float32)).astype(jnp.bfloat16)

    def forward_both(n, s):
        for m in range(2):
            forward(n, m, s)

    def forward_piece(n, p):
        for s in range(1, n_fs):
            forward(n, p, s)

    def spread(n, ks):
        for i, k in enumerate(ks):
            if k:
                arrive(n, k)
            offer(n, k)
            if i:
                reduce(n, ks[i - 1])
        reduce(n, ks[-1])

    middle = n_fs // 2
    for s in range(1, middle + 1):
        forward_both(0, s)
    parts_in(0)
    for p in range(2, carried[0] + 1):
        start_lines(0, p)
    for s in range(middle + 1, n_fs):
        forward_both(0, s)
    for p in range(2, carried[0] + 1):
        forward_piece(0, p)
    part(1, 1).start()
    for m in range(2):
        start_lines(1, m)
        pair(1, m, f).start()
    for p in range(carried[0] + 1, count[0]):
        start_lines(0, p)
    for p in range(carried[0] + 1, count[0]):
        forward_piece(0, p)
    for m in range(2):
        pairs_in(0, m)
    hide(0, normed)
    spread(0, range(steps[0] - 1))
    forward_both(1, 1)
    spread(0, [steps[0] - 1])
    for s in range(2, middle + 1):
        forward_both(1, s)

    def own_prompt(at):
        return prompt[t, :, at].astype(jnp.float32)

    def keep_stream(at, value):
        stream[:, at] = value

    for k in range(steps[0]):
        collect(0, k, own_prompt, keep_stream)
    normed_all[core, seat] = unit(stream[...]).astype(jnp.bfloat16)
    for j in range(pairs - 1):
        give(j).start()
    pass_on(-1).start()
    parts_in(1)
    for p in range(2, count[1]):
        start_lines(1, p)
    for s in range(middle + 1, n_fs):
        forward_both(1, s)
    for j in range(pairs - 1):
        given(j).wait_recv()
        pass_on(j).start()
    for p in range(2, count[1]):
        forward_piece(1, p)
    for j in range(-1, pairs - 1):
        passed_on(j).wait_recv()
    for m in range(2):
        pairs_in(1, m)
    hide(1, normed_all)

    def keep_mixed(at, value):
        mixed_ref[:, at] = value.astype(jnp.bfloat16)

    def own_stream(at):
        return stream[:, at]

    spread(1, range(INSIDE))
    for k in range(INSIDE, steps[1]):
        spread(1, [k])
    drain(0)
    drain(1)
    for k in kernel_groups[1]:
        collect(1, k, own_stream, keep_mixed)
    for j in range(pairs - 1):
        give(j).wait_send()
    for j in range(-1, pairs - 1):
        pass_on(j).wait_send()
    for n in range(2):
        for k in range(steps[n]):
            mate(n, k).wait_send()
            if k in kernel_groups[n]:
                for j in range(pairs - 1):
                    share(n, k, j).wait_send()


def write_kernel(*refs):
    count = (len(refs) - 1) // 2
    sems = refs[-1]
    copies = [
        pltpu.make_async_copy(refs[k], refs[count + k], sems.at[k]) for k in range(count)
    ]
    for copy in copies:
        copy.start()
    for copy in copies:
        copy.wait()


def written(arrays):
    arrays = [pltpu.with_memory_space_constraint(a, pltpu.VMEM) for a in arrays]
    return pl.pallas_call(
        write_kernel,
        out_shape=tuple(jax.ShapeDtypeStruct(a.shape, a.dtype) for a in arrays),
        in_specs=[pl.BlockSpec(memory_space=pltpu.VMEM)] * len(arrays),
        out_specs=(pl.BlockSpec(memory_space=pl.ANY),) * len(arrays),
        scratch_shapes=[pltpu.SemaphoreType.DMA((len(arrays),))],
        compiler_params=pltpu.CompilerParams(vmem_limit_bytes=2**20),
        cost_estimate=pl.CostEstimate(
            flops=2 * 10**9, bytes_accessed=32 * 2**20, transcendentals=0
        ),
    )(*arrays)


def finish_kernel(early_ref, rest_ref, *refs):
    mixed_ref = refs[-1]
    depth = early_ref.shape[1]
    total = rest_ref[...]
    for received in refs[:-1]:
        total += 0.5 * received[...].astype(jnp.float32)
    total = total.astype(mixed_ref.dtype)
    ranges = column_ranges(1, depth, lax.axis_index("gr"))
    done = 0
    for k, columns in enumerate(ranges):
        for at, size in columns:
            at = pl.ds(pl.multiple_of(at, 128), size)
            if k < INSIDE:
                mixed_ref[:, at] = early_ref[:, at]
            else:
                mixed_ref[:, at] = total[:, done : done + size]
                done += size


def finished(early, rest, received):
    return pl.pallas_call(
        finish_kernel,
        out_shape=jax.ShapeDtypeStruct(early.shape, early.dtype),
        compiler_params=pltpu.CompilerParams(vmem_limit_bytes=4 * 2**20),
    )(early, rest, *received)


def fused(sizes, prompt, *weights):
    n_gr, n_fs, n_tp = sizes
    per = n_gr * n_fs // n_tp
    tokens, depth = prompt.shape
    owned = tokens // n_tp
    rows, width = weights[1].shape
    tall, cols = weights[3].shape
    pairs = n_tp // 2
    steps = 1 + max(len(groups) for groups in GROUPS)
    crossing, pieces = sum(map(len, SPLIT)), sum(map(len, SPLIT + SHARED))
    late = sum(size for columns in column_ranges(1, depth, 0)[INSIDE:] for _, size in columns)
    vmem = pl.BlockSpec(memory_space=pltpu.VMEM)
    hbm = pl.BlockSpec(memory_space=pltpu.HBM)
    dma = pltpu.SemaphoreType.DMA
    across = pltpu.VMEM((width, n_gr * n_fs * rows), jnp.bfloat16)
    down = pltpu.VMEM((per, tall, n_tp * cols), jnp.bfloat16)
    operands = [prompt.reshape(n_tp, owned, depth)]
    for n in range(2):
        gain, gate, up, tall_block = weights[4 * n : 4 * n + 4]
        operands += [gain[None, :], gate.T, up.T, tall_block]
    results = pl.pallas_call(
        functools.partial(fused_kernel, n_gr, n_fs, n_tp),
        out_shape=(across, across, down) * 2
        + (
            pltpu.VMEM((owned, depth), jnp.bfloat16),
            pltpu.VMEM((pairs - 1, owned, late), jnp.bfloat16),
            pltpu.VMEM((owned, late), jnp.float32),
        ),
        in_specs=[hbm] * 9,
        out_specs=(vmem,) * 9,
        scratch_shapes=[
            pltpu.VMEM((n_tp, owned, depth), prompt.dtype),
            pltpu.VMEM((2, 1, rows), jnp.float32),
            pltpu.VMEM((2, tall, cols), jnp.float32),
            pltpu.VMEM((4, width, rows), jnp.float32),
            dma((9,)),
            pltpu.VMEM((2, tall, cols), jnp.bfloat16),
            pltpu.VMEM((2, pairs, owned, depth), jnp.bfloat16),
            pltpu.VMEM((2, pairs, owned, depth), jnp.bfloat16),
            pltpu.VMEM((2, pairs * owned, width), jnp.bfloat16),
            pltpu.VMEM((2, pairs * owned, depth), jnp.bfloat16),
            pltpu.VMEM((2, pairs * owned, depth), jnp.bfloat16),
            pltpu.VMEM((2, pairs - 1, owned, depth), jnp.bfloat16),
            pltpu.VMEM((2, pairs - 1, owned, depth), jnp.bfloat16),
            pltpu.VMEM((owned, depth), jnp.float32),
            pltpu.VMEM((owned, depth), jnp.float32),
            dma((4 * (n_fs + 1) + pieces * (per + 1),)),
            dma((4 * n_fs + pieces * per,)),
            dma((4 * n_fs + crossing * per,)),
            dma((4 * n_fs + crossing * per,)),
            dma((2, n_gr)),
            dma((2, n_tp)),
            dma((2, steps)),
            dma((2, steps)),
            dma((2, steps, pairs - 1)),
            dma((2, steps, pairs - 1)),
            dma((2 * pairs - 1,)),
            dma((2 * pairs - 1,)),
        ],
        compiler_params=pltpu.CompilerParams(
            collective_id=2, has_side_effects=True, vmem_limit_bytes=44 * 2**20
        ),
    )(*operands)
    *served, early, sums, rest = results
    received = [
        lax.ppermute(
            sums[j], "tp", [(t, (t + 2 * (1 + j)) % n_tp) for t in range(n_tp)]
        )
        for j in range(pairs - 1)
    ]
    gate_a, up_a, down_a, gate_b, up_b, down_b = written(served)
    mixed = finished(early, rest, received)

    def flat(a):
        return a.reshape(per * tall, n_tp * cols)

    return (gate_a.T, up_a.T, flat(down_a), gate_b.T, up_b.T, flat(down_b), mixed)


def normalize(rows):
    rows = rows.astype(jnp.float32)
    scale = lax.rsqrt(jnp.mean(rows * rows, axis=-1, keepdims=True) + 1e-06)
    return (rows * scale).astype(jnp.bfloat16)


def hidden_units(normed, w_gate, w_up):
    gate = jnp.dot(normed, w_gate, preferred_element_type=jnp.float32)
    upper = jnp.dot(normed, w_up, preferred_element_type=jnp.float32)
    return (jax.nn.silu(gate) * upper).astype(jnp.bfloat16)


def rounded_term(hidden, w_down):
    return jnp.dot(hidden, w_down, preferred_element_type=jnp.float32).astype(jnp.bfloat16)


def suits(sizes, prompt, gate, down):
    n_gr, n_fs, n_tp = sizes
    per = n_gr * n_fs // n_tp
    return (
        n_gr == 2
        and n_tp % 2 == 0
        and per > 0
        and per * n_tp == n_gr * n_fs
        and n_fs % per == 0
        and gate.shape[0] % 128 == 0
        and down.shape[0] % 16 == 0
        and down.shape[1] % 128 == 0
        and prompt.shape[1] % 2048 == 0
        and prompt.shape[0] % (16 * n_tp) == 0
    )


def shards(
    sizes,
    prompt,
    gain_first,
    gate_first,
    up_first,
    down_first,
    gain_second,
    gate_second,
    up_second,
    down_second,
):
    if suits(sizes, prompt, gate_first, down_first):
        return fused(
            sizes,
            prompt,
            gain_first,
            gate_first,
            up_first,
            down_first,
            gain_second,
            gate_second,
            up_second,
            down_second,
        )
    gate_a, up_a, down_a = gather(sizes, 0, gain_first, gate_first, up_first, down_first)
    hidden_a = hidden_units(normalize(prompt), gate_a, up_a)
    term_a = rounded_term(hidden_a, down_a)
    term_a, gain_second = lax.optimization_barrier((term_a, gain_second))
    branch_a = lax.psum(term_a, "tp").astype(jnp.float32)
    gate_b, up_b, down_b = gather(sizes, 1, gain_second, gate_second, up_second, down_second)
    stream = prompt.astype(jnp.float32) + 0.5 * branch_a
    hidden_b = hidden_units(normalize(stream), gate_b, up_b)
    owned = hidden_b.shape[0] // lax.axis_size("tp")
    branch_b = lax.psum_scatter(
        rounded_term(hidden_b, down_b), "tp", scatter_dimension=0, tiled=True
    ).astype(jnp.float32)
    own_stream = lax.dynamic_slice_in_dim(stream, lax.axis_index("tp") * owned, owned, 0)
    mixed = (own_stream + 0.5 * branch_b).astype(jnp.bfloat16)
    return (gate_a, up_a, down_a, gate_b, up_b, down_b, mixed)


def solution(mesh):
    sizes = (mesh.shape["gr"], mesh.shape["fs"], mesh.shape["tp"])
    return jax.shard_map(
        functools.partial(shards, sizes),
        mesh=mesh,
        in_specs=(
            P(("gr", "fs"), None),
            P(("gr", "fs")),
            P(("gr", "fs"), "tp"),
            P(("gr", "fs"), "tp"),
            P(("gr", "fs"), "tp"),
            P(("gr", "fs")),
            P(("gr", "fs"), "tp"),
            P(("gr", "fs"), "tp"),
            P(("gr", "fs"), "tp"),
        ),
        out_specs=(
            P(None, "tp"),
            P(None, "tp"),
            P("tp", None),
            P(None, "tp"),
            P(None, "tp"),
            P("tp", None),
            P(("gr", "fs", "tp"), None),
        ),
        check_vma=False,
    )
```

```python
import functools

import jax
import jax.numpy as jnp
from jax import lax
from jax.experimental import pallas as pl
from jax.experimental.pallas import tpu as pltpu
from jax.sharding import PartitionSpec as P

MESH = pl.DeviceIdType.MESH


def gather_kernel(
    n_gr,
    n_fs,
    n_tp,
    gain_ref,
    gate_ref,
    up_ref,
    down_ref,
    gate_out,
    up_out,
    down_out,
    down_own,
    line_send,
    line_recv,
    pair_send,
    pair_recv,
    part_send,
    part_recv,
):
    g, f, t = lax.axis_index("gr"), lax.axis_index("fs"), lax.axis_index("tp")
    per = n_gr * n_fs // n_tp
    cols = down_ref.shape[1]
    first = lax.rem(t * per, n_fs)
    home = (t * per) // n_fs
    row = g * n_fs + f
    owner = row // per
    slot = lax.rem(row, per)

    width = gate_ref.shape[1]

    def place(ref, origin):
        if len(ref.shape) == 3:
            return ref.at[origin]
        return ref.at[:, pl.ds(pl.multiple_of(origin * width, 128), width)]

    gain = gain_ref[...]
    place(gate_out, row)[...] = (gain * gate_ref[...]).astype(jnp.bfloat16)
    place(up_out, row)[...] = (gain * up_ref[...]).astype(jnp.bfloat16)
    down_own[...] = down_ref[...].astype(jnp.bfloat16)

    @pl.when(owner == t)
    def _():
        down_out[slot, :, pl.ds(pl.multiple_of(t * cols, 128), cols)] = down_ref[...].astype(
            jnp.bfloat16
        )

    barrier = pltpu.get_barrier_semaphore()
    for dg in range(n_gr):
        for dt in range(n_tp):
            if dg or dt:
                pl.semaphore_signal(
                    barrier,
                    inc=1,
                    device_id=(lax.rem(g + dg, n_gr), f, lax.rem(t + dt, n_tp)),
                    device_id_type=MESH,
                )

    for near in (lax.rem(f + 1, n_fs), lax.rem(f + n_fs - 1, n_fs)):
        pl.semaphore_signal(barrier, inc=1, device_id=(g, near, t), device_id_type=MESH)
    pl.semaphore_wait(barrier, n_gr * n_tp + 1)

    outs = (gate_out, up_out)

    def held(o):
        return jnp.logical_and(o >= first, o < first + per)

    def block(m, o):
        if m < 2:
            return place(outs[m], g * n_fs + o)
        return down_out.at[o - first]

    def line(m, way, s):
        step = 1 if way == 0 else -1
        o = f - step * (s - 1)
        return pltpu.make_async_remote_copy(
            src_ref=block(m, o),
            dst_ref=block(m, o),
            send_sem=line_send.at[m, way, s],
            recv_sem=line_recv.at[m, way, s],
            device_id=(g, f + step, t),
            device_id_type=MESH,
        )

    def sends(m, way, s):
        step = 1 if way == 0 else -1
        o = f - step * (s - 1)
        fine = (f < n_fs - 1, o >= 0) if way == 0 else (f > 0, o <= n_fs - 1)
        ok = jnp.logical_and(*fine)
        return jnp.logical_and(ok, held(o)) if m == 2 else ok

    def gets(m, way, s):
        o = f - s if way == 0 else f + s
        ok = o >= 0 if way == 0 else o <= n_fs - 1
        return jnp.logical_and(ok, held(o)) if m == 2 else ok

    def landed(m, way, s):
        o = f - s if way == 0 else f + s
        return pltpu.make_async_remote_copy(
            src_ref=block(m, o),
            dst_ref=block(m, o),
            send_sem=line_send.at[m, way, s],
            recv_sem=line_recv.at[m, way, s],
            device_id=(g, f, t),
            device_id_type=MESH,
        )

    def pair(m, dg, o):
        return pltpu.make_async_remote_copy(
            src_ref=place(outs[m], g * n_fs + o),
            dst_ref=place(outs[m], g * n_fs + o),
            send_sem=pair_send.at[m, dg, o],
            recv_sem=pair_recv.at[m, dg, o],
            device_id=(lax.rem(g + dg, n_gr), f, t),
            device_id_type=MESH,
        )

    def pair_landed(m, dg, o):
        src = lax.rem(g - dg + n_gr, n_gr)
        return pltpu.make_async_remote_copy(
            src_ref=place(outs[m], src * n_fs + o),
            dst_ref=place(outs[m], src * n_fs + o),
            send_sem=pair_send.at[m, dg, o],
            recv_sem=pair_recv.at[m, dg, o],
            device_id=(src, f, t),
            device_id_type=MESH,
        )

    def part(dg):
        to = lax.rem(g + dg, n_gr)
        return pltpu.make_async_remote_copy(
            src_ref=down_own,
            dst_ref=down_out.at[slot, :, pl.ds(pl.multiple_of(t * cols, 128), cols)],
            send_sem=part_send.at[dg],
            recv_sem=part_recv.at[t],
            device_id=(to, f, owner),
            device_id_type=MESH,
        )

    def part_landed(src):
        return pltpu.make_async_remote_copy(
            src_ref=down_own,
            dst_ref=down_out.at[f - first, :, pl.ds(src * cols, cols)],
            send_sem=part_send.at[0],
            recv_sem=part_recv.at[src],
            device_id=(home, f, src),
            device_id_type=MESH,
        )

    for m in range(2):
        for way in range(2):

            @pl.when(sends(m, way, 1))
            def _(m=m, way=way):
                line(m, way, 1).start()

        for dg in range(1, n_gr):
            pair(m, dg, f).start()
    for dg in range(n_gr):
        if dg == 0:

            @pl.when(owner != t)
            def _():
                part(0).start()

        else:
            part(dg).start()

    @pl.when(held(f))
    def _():
        for src in range(n_tp):

            @pl.when(jnp.logical_or(home != g, t != src))
            def _(src=src):
                part_landed(src).wait_recv()

    for way in range(2):

        @pl.when(sends(2, way, 1))
        def _(way=way):
            line(2, way, 1).start()

    for s in range(1, n_fs):
        for m in range(3):
            for way in range(2):

                @pl.when(gets(m, way, s))
                def _(m=m, way=way, s=s):
                    landed(m, way, s).wait_recv()
                    if s < n_fs - 1:

                        @pl.when(sends(m, way, s + 1))
                        def _():
                            line(m, way, s + 1).start()

                    if m < 2:
                        o = f - s if way == 0 else f + s
                        for dg in range(1, n_gr):
                            pair(m, dg, o).start()

    for m in range(2):
        for dg in range(1, n_gr):
            for o in range(n_fs):
                pair_landed(m, dg, o).wait_recv()
                pair(m, dg, o).wait_send()
    for m in range(3):
        for way in range(2):
            for s in range(1, n_fs):

                @pl.when(sends(m, way, s))
                def _(m=m, way=way, s=s):
                    line(m, way, s).wait_send()

    for dg in range(n_gr):
        if dg == 0:

            @pl.when(owner != t)
            def _():
                part(0).wait_send()

        else:
            part(dg).wait_send()


def gather(sizes, call, gain, gate, up, down):
    n_gr, n_fs, n_tp = sizes
    per = n_gr * n_fs // n_tp
    rows, width = gate.shape
    wide = rows % 128 == 0
    whole = (width, n_gr * n_fs * rows) if wide else (n_gr * n_fs, width, rows)
    tall, cols = down.shape
    vmem = pl.BlockSpec(memory_space=pltpu.VMEM)
    dma = pltpu.SemaphoreType.DMA
    gate_all, up_all, down_all = pl.pallas_call(
        functools.partial(gather_kernel, n_gr, n_fs, n_tp),
        out_shape=(
            jax.ShapeDtypeStruct(whole, jnp.bfloat16),
            jax.ShapeDtypeStruct(whole, jnp.bfloat16),
            jax.ShapeDtypeStruct((per, tall, n_tp * cols), jnp.bfloat16),
        ),
        in_specs=[vmem] * 4,
        out_specs=(vmem,) * 3,
        scratch_shapes=[
            pltpu.VMEM((tall, cols), jnp.bfloat16),
            dma((3, 2, n_fs)),
            dma((3, 2, n_fs)),
            dma((2, n_gr, n_fs)),
            dma((2, n_gr, n_fs)),
            dma((n_gr,)),
            dma((n_tp,)),
        ],
        compiler_params=pltpu.CompilerParams(
            collective_id=call, has_side_effects=True, vmem_limit_bytes=32 * 2**20
        ),
        cost_estimate=pl.CostEstimate(
            flops=10**10, bytes_accessed=16 * 2**20, transcendentals=0
        ),
    )(gain[None, :], gate.T, up.T, down)

    def upright(a):
        return a.T if wide else a.transpose(0, 2, 1).reshape(n_gr * n_fs * rows, width)

    return (
        upright(gate_all),
        upright(up_all),
        down_all.reshape(per * tall, n_tp * cols),
    )


SPLIT = ((3,), (3, 1, 1))
SHARED = ((5, 5), (4, 1, 1))
GROUPS = (
    (((0,), ()), ((1,), (0,))),
    (((0,), ()), ((1,), (0,)), ((2,), (1, 2))),
)


def laid(start, sizes):
    return tuple((start + sum(sizes[:i]), size) for i, size in enumerate(sizes))


def down_pieces(n, depth, column):
    unit = depth // 16
    split = [unit * size for size in SPLIT[n]]
    shared = [unit * size for size in SHARED[n]]
    return laid(sum(shared) + column * sum(split), split), laid(0, shared)


def column_ranges(n, depth, g):
    own, shared = down_pieces(n, depth, g)
    other, _ = down_pieces(n, depth, 1 - g)
    ranges = [((own[0][0], sum(size for _, size in own)),)]
    for whole, pieces in GROUPS[n]:
        ranges.append(tuple(shared[i] for i in whole) + tuple(other[i] for i in pieces))
    return ranges


INSIDE = 2


def fused_kernel(
    n_gr,
    n_fs,
    n_tp,
    prompt_in,
    gain_in_a,
    gate_in_a,
    up_in_a,
    down_in_a,
    gain_in_b,
    gate_in_b,
    up_in_b,
    down_in_b,
    gate_out_a,
    up_out_a,
    down_out_a,
    gate_out_b,
    up_out_b,
    down_out_b,
    mixed_ref,
    late_sums,
    late_rest,
    prompt,
    gains,
    tall_in,
    gates_in,
    load_sem,
    down_own,
    normed,
    normed_all,
    hidden,
    mate_out,
    mate_in,
    sums,
    sums_in,
    kept,
    stream,
    line_send,
    line_recv,
    pair_send,
    pair_recv,
    part_send,
    part_recv,
    mate_send,
    mate_recv,
    sum_send,
    sum_recv,
    row_send,
    row_recv,
):
    g, f, t = lax.axis_index("gr"), lax.axis_index("fs"), lax.axis_index("tp")
    per = n_gr * n_fs // n_tp
    tall, cols = down_in_a.shape
    width = gate_in_a.shape[1]
    owned, depth = prompt.shape[1], prompt.shape[2]
    first = lax.rem(t * per, n_fs)
    home = (t * per) // n_fs
    row = g * n_fs + f
    owner = row // per
    slot = lax.rem(row, per)
    pairs = n_tp // 2
    seat, core = t // 2, lax.rem(t, 2)
    outs = ((gate_out_a, up_out_a, down_out_a), (gate_out_b, up_out_b, down_out_b))

    carried = [2 + len(split) for split in SPLIT]
    count = [c + len(shared) for c, shared in zip(carried, SHARED)]

    def lanes(at, size):
        return pl.ds(pl.multiple_of(at, 128), size)

    loads = []
    for k, (src, dst) in enumerate(
        (
            (gain_in_a, gains.at[0]),
            (gate_in_a, gates_in.at[0]),
            (up_in_a, gates_in.at[1]),
            (down_in_a, tall_in.at[0]),
            (prompt_in, prompt),
            (gain_in_b, gains.at[1]),
            (down_in_b, tall_in.at[1]),
            (gate_in_b, gates_in.at[2]),
            (up_in_b, gates_in.at[3]),
        )
    ):
        load = pltpu.make_async_copy(src, dst, load_sem.at[k])
        load.start()
        loads.append(load)

    barrier = pltpu.get_barrier_semaphore()
    for dg in range(n_gr):
        for dt in range(n_tp):
            if dg or dt:
                pl.semaphore_signal(
                    barrier,
                    inc=1,
                    device_id=(lax.rem(g + dg, n_gr), f, lax.rem(t + dt, n_tp)),
                    device_id_type=MESH,
                )
    for near, there in ((f + 1, f < n_fs - 1), (f - 1, f > 0)):

        @pl.when(there)
        def _(near=near):
            pl.semaphore_signal(barrier, inc=1, device_id=(g, near, t), device_id_type=MESH)

    between = jnp.logical_and(f > 0, f < n_fs - 1)
    greeted = n_gr * n_tp + jnp.where(between, 1, 0)

    def place(ref, origin):
        return ref.at[:, pl.ds(pl.multiple_of(origin * width, 128), width)]

    def round_matrix(n, m):
        place(outs[n][m], row)[...] = (gains[n] * gates_in[2 * n + m]).astype(jnp.bfloat16)

    def round_down(n):
        rounded = tall_in[n].astype(jnp.bfloat16)
        down_own[n] = rounded

        @pl.when(owner == t)
        def _():
            outs[n][2][slot, :, lanes(t * cols, cols)] = rounded

    def held(o):
        return jnp.logical_and(o >= first, o < first + per)

    def remote(src, dst, send, recv, to):
        return pltpu.make_async_remote_copy(
            src_ref=src,
            dst_ref=dst,
            send_sem=send,
            recv_sem=recv,
            device_id=to,
            device_id_type=MESH,
        )

    def spot(n, p, o, column):
        if p < 2:
            return place(outs[n][p], column * n_fs + o)
        split, shared = down_pieces(n, depth, column)
        at, size = (split + shared)[p - 2]
        return outs[n][2].at[o - first, :, lanes(at, size)]

    def down_index(n, p):
        return n * (count[0] - 2) + p - 2

    def send_seat(n, p, o):
        if p < 2:
            return 2 * n + p
        return 4 + down_index(n, p) * (per + 1) + o - first

    def recv_seat(n, p, o):
        if p < 2:
            return (2 * n + p) * n_fs + o
        return 4 * n_fs + down_index(n, p) * per + o - first

    def line_sems(n, p, way, s, o):
        own = per + first if s == 1 and way == 1 else o
        return line_send.at[send_seat(n, p, own)], line_recv.at[recv_seat(n, p, o)]

    def line(n, p, way, s):
        step = 1 if way == 0 else -1
        o = f - step * (s - 1)
        sems = line_sems(n, p, way, s, o)
        return remote(spot(n, p, o, g), spot(n, p, o, g), *sems, (g, f + step, t))

    def sends(p, way, s):
        step = 1 if way == 0 else -1
        o = f - step * (s - 1)
        fine = (f < n_fs - 1, o >= 0) if way == 0 else (f > 0, o <= n_fs - 1)
        ok = jnp.logical_and(*fine)
        return jnp.logical_and(ok, held(o)) if p >= 2 else ok

    def origin(way, s):
        return f - s if way == 0 else f + s

    def gets(p, way, s):
        o = origin(way, s)
        ok = o >= 0 if way == 0 else o <= n_fs - 1
        return jnp.logical_and(ok, held(o)) if p >= 2 else ok

    def ends(way):
        return f == n_fs - 1 if way == 0 else f == 0

    def landed(n, p, way, s):
        o = origin(way, s)
        sems = line_sems(n, p, 0, s, o)
        return remote(spot(n, p, o, g), spot(n, p, o, g), *sems, (g, f, t))

    def pair_seat(n, p, o):
        if p < 2:
            return 2 * n + p
        return 4 + (n * (carried[0] - 2) + p - 2) * per + o - first

    def pair(n, p, o):
        sems = pair_send.at[pair_seat(n, p, o)], pair_recv.at[pair_seat(n, p, o)]
        return remote(spot(n, p, o, g), spot(n, p, o, g), *sems, (1 - g, f, t))

    def pair_landed(n, p, o):
        sems = pair_send.at[pair_seat(n, p, o)], pair_recv.at[pair_seat(n, p, o)]
        return remote(spot(n, p, o, 1 - g), spot(n, p, o, 1 - g), *sems, (1 - g, f, t))

    def part(n, dg):
        return remote(
            down_own.at[n],
            outs[n][2].at[slot, :, lanes(t * cols, cols)],
            part_send.at[n, dg],
            part_recv.at[n, t],
            (lax.rem(g + dg, n_gr), f, owner),
        )

    def part_landed(n, src):
        return remote(
            down_own.at[n],
            outs[n][2].at[f - first, :, pl.ds(src * cols, cols)],
            part_send.at[n, 0],
            part_recv.at[n, src],
            (home, f, src),
        )

    def start_lines(n, p):
        for way in range(2):

            @pl.when(sends(p, way, 1))
            def _(way=way):
                line(n, p, way, 1).start()

    def give_part(n):
        @pl.when(owner != t)
        def _():
            part(n, 0).start()

    def parts_in(n):
        @pl.when(held(f))
        def _():
            for src in range(n_tp):

                @pl.when(jnp.logical_or(home != g, t != src))
                def _(src=src):
                    part_landed(n, src).wait_recv()

    def forward(n, p, s):
        crosses, relays = p < carried[n], s < n_fs - 1
        for way in range(2):
            if not crosses and not relays:
                continue
            ready = gets(p, way, s)
            if not crosses:
                ready = jnp.logical_and(ready, jnp.logical_not(ends(way)))

            @pl.when(ready)
            def _(way=way):
                landed(n, p, way, s).wait_recv()
                if relays:

                    @pl.when(sends(p, way, s + 1))
                    def _():
                        line(n, p, way, s + 1).start()

                if crosses:
                    pair(n, p, origin(way, s)).start()

    def settle(n, p):
        for s in range(1, n_fs):
            for way in range(2):
                ready = gets(p, way, s)
                if s < n_fs - 1:
                    ready = jnp.logical_and(ready, ends(way))

                @pl.when(ready)
                def _(way=way, s=s):
                    landed(n, p, way, s).wait_recv()

    def blocks(n, p, origin, many, send, recv):
        at = pl.ds(pl.multiple_of(origin * width, 128), many * width)
        spot = outs[n][p].at[:, at]
        return remote(spot, spot, send, recv, (1 - g, f, t))

    def pair_blocks(n, p, column):
        sems = pair_send.at[pair_seat(n, p, 0)], pair_recv.at[pair_seat(n, p, 0)]
        return blocks(n, p, column * n_fs, n_fs, *sems)

    def pairs_in(n, p):
        if p < 2:
            pair_blocks(n, p, 1 - g).wait_recv()
            return
        for o in range(n_fs):

            @pl.when(jnp.logical_and(held(o), o != f))
            def _(o=o):
                pair_landed(n, p, o).wait_recv()

    def drain(n):
        for p in range(2):
            pair_blocks(n, p, g).wait_send()
            sems = line_send.at[send_seat(n, p, 0)], line_recv.at[recv_seat(n, p, 0)]

            @pl.when(between)
            def _(p=p, sems=sems):
                blocks(n, p, 0, n_fs + 1, *sems).wait_send()

            @pl.when(jnp.logical_not(between))
            def _(p=p, sems=sems):
                blocks(n, p, 0, 1, *sems).wait_send()

        for p in range(2, carried[n]):
            for o in range(n_fs):

                @pl.when(jnp.logical_and(held(o), o != f))
                def _(p=p, o=o):
                    pair(n, p, o).wait_send()

        for p in range(2, count[n]):
            for way in range(2):
                for s in range(1, n_fs):

                    @pl.when(sends(p, way, s))
                    def _(p=p, way=way, s=s):
                        line(n, p, way, s).wait_send()

        @pl.when(owner != t)
        def _():
            part(n, 0).wait_send()

        part(n, 1).wait_send()

    across = (((1,), (1,)), ((), ()))

    def unit(rows):
        return rows * lax.rsqrt(jnp.mean(rows * rows, axis=-1, keepdims=True) + 1e-06)

    def seat_of(j):
        return lax.rem(seat + 1 + j, pairs)

    def hide(n, source):
        @pl.loop(0, 2)
        def _(c):
            rows = jnp.concatenate([source[c, seat_of(j)] for j in range(pairs)], axis=0)
            gate = lax.dot_general(
                rows, outs[n][0][...], across, preferred_element_type=jnp.float32
            )
            upper = lax.dot_general(
                rows, outs[n][1][...], across, preferred_element_type=jnp.float32
            )
            hidden[c] = (jax.nn.silu(gate) * upper).astype(jnp.bfloat16)

    ranges = [column_ranges(n, depth, g) for n in range(2)]
    steps = [len(part) for part in ranges]
    widths = [[sum(size for _, size in columns) for columns in part] for part in ranges]
    starts = [[sum(sizes[:k]) for k in range(len(sizes))] for sizes in widths]
    spans = [[pl.ds(*at) for at in zip(starts[n], widths[n])] for n in range(2)]
    kernel_groups = (range(steps[0]), range(INSIDE))

    def mate(n, k):
        at = spans[n][k]
        return remote(
            mate_out.at[n, :, at],
            mate_in.at[n, :, at],
            mate_send.at[n],
            mate_recv.at[n, k],
            (g, f, t + 1 - 2 * core),
        )

    def share(n, k, j):
        at = spans[n][k]
        return remote(
            sums.at[n, j, :, at],
            sums_in.at[n, j, :, at],
            sum_send.at[n, j],
            sum_recv.at[n, k, j],
            (g, f, 2 * seat_of(j) + core),
        )

    def term(n, units, k):
        tiles = [
            jnp.dot(
                units,
                outs[n][2][:, :, lanes(at, size)].reshape(per * tall, size),
                preferred_element_type=jnp.float32,
            )
            for at, size in ranges[n][k]
        ]
        return tiles[0] if len(tiles) == 1 else jnp.concatenate(tiles, axis=1)

    def arrive(n, k):
        whole, pieces = GROUPS[n][k - 1]
        for i in whole:
            settle(n, carried[n] + i)
        for i in pieces:
            pairs_in(n, 2 + i)

    def offer(n, k):
        mate_out[n, :, spans[n][k]] = term(n, hidden[1 - core], k).astype(jnp.bfloat16)
        mate(n, k).start()

    def reduce(n, k):
        at = spans[n][k]
        mine = term(n, hidden[core], k)
        mate(n, k).wait_recv()
        both = mine + mate_in[n, :, at].astype(jnp.float32)
        if k in kernel_groups[n]:
            for j in range(pairs - 1):
                sums[n, j, :, at] = both[j * owned : (j + 1) * owned].astype(jnp.bfloat16)
                share(n, k, j).start()
            kept[:, at] = both[(pairs - 1) * owned :]
            return
        late = starts[n][k] - starts[n][INSIDE]
        for j in range(pairs - 1):
            late_sums[j, :, pl.ds(late, widths[n][k])] = both[j * owned : (j + 1) * owned].astype(
                jnp.bfloat16
            )
        passed = (pairs - 1) * owned
        done = 0
        for column, size in ranges[n][k]:
            late_rest[:, pl.ds(late + done, size)] = (
                stream[:, lanes(column, size)] + 0.5 * both[passed:, done : done + size]
            )
            done += size

    def collect(n, k, base, finish):
        for j in range(pairs - 1):
            share(n, k, j).wait_recv()
        total = kept[:, spans[n][k]]
        for j in range(pairs - 1):
            total += sums_in[n, j, :, spans[n][k]].astype(jnp.float32)
        passed = 0
        for at, size in ranges[n][k]:
            finish(lanes(at, size), base(lanes(at, size)) + 0.5 * total[:, passed : passed + size])
            passed += size

    def give(j):
        own = normed_all.at[core, seat]
        return remote(own, own, row_send.at[j], row_recv.at[j], (g, f, 2 * seat_of(j) + core))

    def given(j):
        src = lax.rem(seat - 1 - j + pairs, pairs)
        spot = normed_all.at[core, src]
        return remote(spot, spot, row_send.at[j], row_recv.at[j], (g, f, 2 * src + core))

    def pass_on(j):
        src = lax.rem(seat - 1 - j + 2 * pairs, pairs)
        spot = normed_all.at[core, src]
        at = pairs - 1 + (pairs - 1 if j < 0 else j)
        return remote(
            spot, spot, row_send.at[at], row_recv.at[at], (g, f, t + 1 - 2 * core)
        )

    def passed_on(j):
        src = lax.rem(seat - 1 - j + 2 * pairs, pairs)
        spot = normed_all.at[1 - core, src]
        at = pairs - 1 + (pairs - 1 if j < 0 else j)
        return remote(
            spot, spot, row_send.at[at], row_recv.at[at], (g, f, t + 1 - 2 * core)
        )

    loads[0].wait()
    loads[1].wait()
    round_matrix(0, 0)
    pl.semaphore_wait(barrier, greeted)
    start_lines(0, 0)
    pair(0, 0, f).start()
    loads[2].wait()
    round_matrix(0, 1)
    start_lines(0, 1)
    pair(0, 1, f).start()
    loads[3].wait()
    round_down(0)
    part(0, 1).start()
    give_part(0)
    loads[5].wait()
    loads[6].wait()
    round_down(1)
    give_part(1)
    loads[7].wait()
    round_matrix(1, 0)
    loads[8].wait()
    round_matrix(1, 1)
    loads[4].wait()

    @pl.loop(0, n_tp)
    def _(i):
        normed[lax.rem(i, 2), i // 2] = unit(prompt[i].astype(jnp.float32)).astype(jnp.bfloat16)

    def forward_both(n, s):
        for m in range(2):
            forward(n, m, s)

    def forward_piece(n, p):
        for s in range(1, n_fs):
            forward(n, p, s)

    def spread(n, ks):
        for i, k in enumerate(ks):
            if k:
                arrive(n, k)
            offer(n, k)
            if i:
                reduce(n, ks[i - 1])
        reduce(n, ks[-1])

    middle = n_fs // 2
    for s in range(1, middle + 1):
        forward_both(0, s)
    parts_in(0)
    for p in range(2, carried[0] + 1):
        start_lines(0, p)
    for s in range(middle + 1, n_fs):
        forward_both(0, s)
    for p in range(2, carried[0] + 1):
        forward_piece(0, p)
    part(1, 1).start()
    for m in range(2):
        start_lines(1, m)
        pair(1, m, f).start()
    for p in range(carried[0] + 1, count[0]):
        start_lines(0, p)
    for p in range(carried[0] + 1, count[0]):
        forward_piece(0, p)
    for m in range(2):
        pairs_in(0, m)
    hide(0, normed)
    spread(0, range(steps[0] - 1))
    forward_both(1, 1)
    spread(0, [steps[0] - 1])
    for s in range(2, middle + 1):
        forward_both(1, s)

    def own_prompt(at):
        return prompt[t, :, at].astype(jnp.float32)

    def keep_stream(at, value):
        stream[:, at] = value

    for k in range(steps[0]):
        collect(0, k, own_prompt, keep_stream)
    normed_all[core, seat] = unit(stream[...]).astype(jnp.bfloat16)
    for j in range(pairs - 1):
        give(j).start()
    pass_on(-1).start()
    parts_in(1)
    for p in range(2, count[1]):
        start_lines(1, p)
    for s in range(middle + 1, n_fs):
        forward_both(1, s)
    for j in range(pairs - 1):
        given(j).wait_recv()
        pass_on(j).start()
    for p in range(2, count[1]):
        forward_piece(1, p)
    for j in range(-1, pairs - 1):
        passed_on(j).wait_recv()
    for m in range(2):
        pairs_in(1, m)
    hide(1, normed_all)

    def keep_mixed(at, value):
        mixed_ref[:, at] = value.astype(jnp.bfloat16)

    def own_stream(at):
        return stream[:, at]

    for k in range(steps[1]):
        spread(1, [k])
    drain(0)
    drain(1)
    for k in kernel_groups[1]:
        collect(1, k, own_stream, keep_mixed)
    for j in range(pairs - 1):
        give(j).wait_send()
    for j in range(-1, pairs - 1):
        pass_on(j).wait_send()
    for n in range(2):
        spot = mate_out.at[n]
        remote(
            spot, spot, mate_send.at[n], mate_recv.at[n, 0], (g, f, t + 1 - 2 * core)
        ).wait_send()
        whole = pl.ds(0, sum(widths[n][k] for k in kernel_groups[n]))
        for j in range(pairs - 1):
            spot = sums.at[n, j, :, whole]
            remote(
                spot, spot, sum_send.at[n, j], sum_recv.at[n, 0, j], (g, f, 2 * seat_of(j) + core)
            ).wait_send()


def write_kernel(*refs):
    count = (len(refs) - 1) // 2
    sems = refs[-1]
    copies = [
        pltpu.make_async_copy(refs[k], refs[count + k], sems.at[k]) for k in range(count)
    ]
    for copy in copies:
        copy.start()
    for copy in copies:
        copy.wait()


def written(arrays):
    arrays = [pltpu.with_memory_space_constraint(a, pltpu.VMEM) for a in arrays]
    return pl.pallas_call(
        write_kernel,
        out_shape=tuple(jax.ShapeDtypeStruct(a.shape, a.dtype) for a in arrays),
        in_specs=[pl.BlockSpec(memory_space=pltpu.VMEM)] * len(arrays),
        out_specs=(pl.BlockSpec(memory_space=pl.ANY),) * len(arrays),
        scratch_shapes=[pltpu.SemaphoreType.DMA((len(arrays),))],
        compiler_params=pltpu.CompilerParams(vmem_limit_bytes=2**20),
        cost_estimate=pl.CostEstimate(
            flops=2 * 10**9, bytes_accessed=32 * 2**20, transcendentals=0
        ),
    )(*arrays)


def finish_kernel(early_ref, rest_ref, *refs):
    mixed_ref = refs[-1]
    depth = early_ref.shape[1]
    total = rest_ref[...]
    for received in refs[:-1]:
        total += 0.5 * received[...].astype(jnp.float32)
    total = total.astype(mixed_ref.dtype)
    ranges = column_ranges(1, depth, lax.axis_index("gr"))
    done = 0
    for k, columns in enumerate(ranges):
        for at, size in columns:
            at = pl.ds(pl.multiple_of(at, 128), size)
            if k < INSIDE:
                mixed_ref[:, at] = early_ref[:, at]
            else:
                mixed_ref[:, at] = total[:, done : done + size]
                done += size


def finished(early, rest, received):
    return pl.pallas_call(
        finish_kernel,
        out_shape=jax.ShapeDtypeStruct(early.shape, early.dtype),
        compiler_params=pltpu.CompilerParams(vmem_limit_bytes=4 * 2**20),
    )(early, rest, *received)


def fused(sizes, prompt, *weights):
    n_gr, n_fs, n_tp = sizes
    per = n_gr * n_fs // n_tp
    tokens, depth = prompt.shape
    owned = tokens // n_tp
    rows, width = weights[1].shape
    tall, cols = weights[3].shape
    pairs = n_tp // 2
    steps = 1 + max(len(groups) for groups in GROUPS)
    crossing, pieces = sum(map(len, SPLIT)), sum(map(len, SPLIT + SHARED))
    late = sum(size for columns in column_ranges(1, depth, 0)[INSIDE:] for _, size in columns)
    vmem = pl.BlockSpec(memory_space=pltpu.VMEM)
    hbm = pl.BlockSpec(memory_space=pltpu.HBM)
    dma = pltpu.SemaphoreType.DMA
    across = pltpu.VMEM((width, n_gr * n_fs * rows), jnp.bfloat16)
    down = pltpu.VMEM((per, tall, n_tp * cols), jnp.bfloat16)
    operands = [prompt.reshape(n_tp, owned, depth)]
    for n in range(2):
        gain, gate, up, tall_block = weights[4 * n : 4 * n + 4]
        operands += [gain[None, :], gate.T, up.T, tall_block]
    results = pl.pallas_call(
        functools.partial(fused_kernel, n_gr, n_fs, n_tp),
        out_shape=(across, across, down) * 2
        + (
            pltpu.VMEM((owned, depth), jnp.bfloat16),
            pltpu.VMEM((pairs - 1, owned, late), jnp.bfloat16),
            pltpu.VMEM((owned, late), jnp.float32),
        ),
        in_specs=[hbm] * 9,
        out_specs=(vmem,) * 9,
        scratch_shapes=[
            pltpu.VMEM((n_tp, owned, depth), prompt.dtype),
            pltpu.VMEM((2, 1, rows), jnp.float32),
            pltpu.VMEM((2, tall, cols), jnp.float32),
            pltpu.VMEM((4, width, rows), jnp.float32),
            dma((9,)),
            pltpu.VMEM((2, tall, cols), jnp.bfloat16),
            pltpu.VMEM((2, pairs, owned, depth), jnp.bfloat16),
            pltpu.VMEM((2, pairs, owned, depth), jnp.bfloat16),
            pltpu.VMEM((2, pairs * owned, width), jnp.bfloat16),
            pltpu.VMEM((2, pairs * owned, depth), jnp.bfloat16),
            pltpu.VMEM((2, pairs * owned, depth), jnp.bfloat16),
            pltpu.VMEM((2, pairs - 1, owned, depth), jnp.bfloat16),
            pltpu.VMEM((2, pairs - 1, owned, depth), jnp.bfloat16),
            pltpu.VMEM((owned, depth), jnp.float32),
            pltpu.VMEM((owned, depth), jnp.float32),
            dma((4 + pieces * (per + 1),)),
            dma((4 * n_fs + pieces * per,)),
            dma((4 + crossing * per,)),
            dma((4 + crossing * per,)),
            dma((2, n_gr)),
            dma((2, n_tp)),
            dma((2,)),
            dma((2, steps)),
            dma((2, pairs - 1)),
            dma((2, steps, pairs - 1)),
            dma((2 * pairs - 1,)),
            dma((2 * pairs - 1,)),
        ],
        compiler_params=pltpu.CompilerParams(
            collective_id=2, has_side_effects=True, vmem_limit_bytes=44 * 2**20
        ),
    )(*operands)
    *served, early, sums, rest = results
    received = [
        lax.ppermute(
            sums[j], "tp", [(t, (t + 2 * (1 + j)) % n_tp) for t in range(n_tp)]
        )
        for j in range(pairs - 1)
    ]
    gate_a, up_a, down_a, gate_b, up_b, down_b = written(served)
    mixed = finished(early, rest, received)

    def flat(a):
        return a.reshape(per * tall, n_tp * cols)

    return (gate_a.T, up_a.T, flat(down_a), gate_b.T, up_b.T, flat(down_b), mixed)


def normalize(rows):
    rows = rows.astype(jnp.float32)
    scale = lax.rsqrt(jnp.mean(rows * rows, axis=-1, keepdims=True) + 1e-06)
    return (rows * scale).astype(jnp.bfloat16)


def hidden_units(normed, w_gate, w_up):
    gate = jnp.dot(normed, w_gate, preferred_element_type=jnp.float32)
    upper = jnp.dot(normed, w_up, preferred_element_type=jnp.float32)
    return (jax.nn.silu(gate) * upper).astype(jnp.bfloat16)


def rounded_term(hidden, w_down):
    return jnp.dot(hidden, w_down, preferred_element_type=jnp.float32).astype(jnp.bfloat16)


def suits(sizes, prompt, gate, down):
    n_gr, n_fs, n_tp = sizes
    per = n_gr * n_fs // n_tp
    return (
        n_gr == 2
        and n_tp % 2 == 0
        and per > 0
        and per * n_tp == n_gr * n_fs
        and n_fs % per == 0
        and gate.shape[0] % 128 == 0
        and down.shape[0] % 16 == 0
        and down.shape[1] % 128 == 0
        and prompt.shape[1] % 2048 == 0
        and prompt.shape[0] % (16 * n_tp) == 0
    )


def shards(
    sizes,
    prompt,
    gain_first,
    gate_first,
    up_first,
    down_first,
    gain_second,
    gate_second,
    up_second,
    down_second,
):
    if suits(sizes, prompt, gate_first, down_first):
        return fused(
            sizes,
            prompt,
            gain_first,
            gate_first,
            up_first,
            down_first,
            gain_second,
            gate_second,
            up_second,
            down_second,
        )
    gate_a, up_a, down_a = gather(sizes, 0, gain_first, gate_first, up_first, down_first)
    hidden_a = hidden_units(normalize(prompt), gate_a, up_a)
    term_a = rounded_term(hidden_a, down_a)
    term_a, gain_second = lax.optimization_barrier((term_a, gain_second))
    branch_a = lax.psum(term_a, "tp").astype(jnp.float32)
    gate_b, up_b, down_b = gather(sizes, 1, gain_second, gate_second, up_second, down_second)
    stream = prompt.astype(jnp.float32) + 0.5 * branch_a
    hidden_b = hidden_units(normalize(stream), gate_b, up_b)
    owned = hidden_b.shape[0] // lax.axis_size("tp")
    branch_b = lax.psum_scatter(
        rounded_term(hidden_b, down_b), "tp", scatter_dimension=0, tiled=True
    ).astype(jnp.float32)
    own_stream = lax.dynamic_slice_in_dim(stream, lax.axis_index("tp") * owned, owned, 0)
    mixed = (own_stream + 0.5 * branch_b).astype(jnp.bfloat16)
    return (gate_a, up_a, down_a, gate_b, up_b, down_b, mixed)


def solution(mesh):
    sizes = (mesh.shape["gr"], mesh.shape["fs"], mesh.shape["tp"])
    return jax.shard_map(
        functools.partial(shards, sizes),
        mesh=mesh,
        in_specs=(
            P(("gr", "fs"), None),
            P(("gr", "fs")),
            P(("gr", "fs"), "tp"),
            P(("gr", "fs"), "tp"),
            P(("gr", "fs"), "tp"),
            P(("gr", "fs")),
            P(("gr", "fs"), "tp"),
            P(("gr", "fs"), "tp"),
            P(("gr", "fs"), "tp"),
        ),
        out_specs=(
            P(None, "tp"),
            P(None, "tp"),
            P("tp", None),
            P(None, "tp"),
            P(None, "tp"),
            P("tp", None),
            P(("gr", "fs", "tp"), None),
        ),
        check_vma=False,
    )
```

```python
import functools

import jax
import jax.numpy as jnp
from jax import lax
from jax.experimental import pallas as pl
from jax.experimental.pallas import tpu as pltpu
from jax.sharding import PartitionSpec as P

MESH = pl.DeviceIdType.MESH


def gather_kernel(
    n_gr,
    n_fs,
    n_tp,
    gain_ref,
    gate_ref,
    up_ref,
    down_ref,
    gate_out,
    up_out,
    down_out,
    down_own,
    line_send,
    line_recv,
    pair_send,
    pair_recv,
    part_send,
    part_recv,
):
    g, f, t = lax.axis_index("gr"), lax.axis_index("fs"), lax.axis_index("tp")
    per = n_gr * n_fs // n_tp
    cols = down_ref.shape[1]
    first = lax.rem(t * per, n_fs)
    home = (t * per) // n_fs
    row = g * n_fs + f
    owner = row // per
    slot = lax.rem(row, per)

    width = gate_ref.shape[1]

    def place(ref, origin):
        if len(ref.shape) == 3:
            return ref.at[origin]
        return ref.at[:, pl.ds(pl.multiple_of(origin * width, 128), width)]

    gain = gain_ref[...]
    place(gate_out, row)[...] = (gain * gate_ref[...]).astype(jnp.bfloat16)
    place(up_out, row)[...] = (gain * up_ref[...]).astype(jnp.bfloat16)
    down_own[...] = down_ref[...].astype(jnp.bfloat16)

    @pl.when(owner == t)
    def _():
        down_out[slot, :, pl.ds(pl.multiple_of(t * cols, 128), cols)] = down_ref[...].astype(
            jnp.bfloat16
        )

    barrier = pltpu.get_barrier_semaphore()
    for dg in range(n_gr):
        for dt in range(n_tp):
            if dg or dt:
                pl.semaphore_signal(
                    barrier,
                    inc=1,
                    device_id=(lax.rem(g + dg, n_gr), f, lax.rem(t + dt, n_tp)),
                    device_id_type=MESH,
                )

    for near in (lax.rem(f + 1, n_fs), lax.rem(f + n_fs - 1, n_fs)):
        pl.semaphore_signal(barrier, inc=1, device_id=(g, near, t), device_id_type=MESH)
    pl.semaphore_wait(barrier, n_gr * n_tp + 1)

    outs = (gate_out, up_out)

    def held(o):
        return jnp.logical_and(o >= first, o < first + per)

    def block(m, o):
        if m < 2:
            return place(outs[m], g * n_fs + o)
        return down_out.at[o - first]

    def line(m, way, s):
        step = 1 if way == 0 else -1
        o = f - step * (s - 1)
        return pltpu.make_async_remote_copy(
            src_ref=block(m, o),
            dst_ref=block(m, o),
            send_sem=line_send.at[m, way, s],
            recv_sem=line_recv.at[m, way, s],
            device_id=(g, f + step, t),
            device_id_type=MESH,
        )

    def sends(m, way, s):
        step = 1 if way == 0 else -1
        o = f - step * (s - 1)
        fine = (f < n_fs - 1, o >= 0) if way == 0 else (f > 0, o <= n_fs - 1)
        ok = jnp.logical_and(*fine)
        return jnp.logical_and(ok, held(o)) if m == 2 else ok

    def gets(m, way, s):
        o = f - s if way == 0 else f + s
        ok = o >= 0 if way == 0 else o <= n_fs - 1
        return jnp.logical_and(ok, held(o)) if m == 2 else ok

    def landed(m, way, s):
        o = f - s if way == 0 else f + s
        return pltpu.make_async_remote_copy(
            src_ref=block(m, o),
            dst_ref=block(m, o),
            send_sem=line_send.at[m, way, s],
            recv_sem=line_recv.at[m, way, s],
            device_id=(g, f, t),
            device_id_type=MESH,
        )

    def pair(m, dg, o):
        return pltpu.make_async_remote_copy(
            src_ref=place(outs[m], g * n_fs + o),
            dst_ref=place(outs[m], g * n_fs + o),
            send_sem=pair_send.at[m, dg, o],
            recv_sem=pair_recv.at[m, dg, o],
            device_id=(lax.rem(g + dg, n_gr), f, t),
            device_id_type=MESH,
        )

    def pair_landed(m, dg, o):
        src = lax.rem(g - dg + n_gr, n_gr)
        return pltpu.make_async_remote_copy(
            src_ref=place(outs[m], src * n_fs + o),
            dst_ref=place(outs[m], src * n_fs + o),
            send_sem=pair_send.at[m, dg, o],
            recv_sem=pair_recv.at[m, dg, o],
            device_id=(src, f, t),
            device_id_type=MESH,
        )

    def part(dg):
        to = lax.rem(g + dg, n_gr)
        return pltpu.make_async_remote_copy(
            src_ref=down_own,
            dst_ref=down_out.at[slot, :, pl.ds(pl.multiple_of(t * cols, 128), cols)],
            send_sem=part_send.at[dg],
            recv_sem=part_recv.at[t],
            device_id=(to, f, owner),
            device_id_type=MESH,
        )

    def part_landed(src):
        return pltpu.make_async_remote_copy(
            src_ref=down_own,
            dst_ref=down_out.at[f - first, :, pl.ds(src * cols, cols)],
            send_sem=part_send.at[0],
            recv_sem=part_recv.at[src],
            device_id=(home, f, src),
            device_id_type=MESH,
        )

    for m in range(2):
        for way in range(2):

            @pl.when(sends(m, way, 1))
            def _(m=m, way=way):
                line(m, way, 1).start()

        for dg in range(1, n_gr):
            pair(m, dg, f).start()
    for dg in range(n_gr):
        if dg == 0:

            @pl.when(owner != t)
            def _():
                part(0).start()

        else:
            part(dg).start()

    @pl.when(held(f))
    def _():
        for src in range(n_tp):

            @pl.when(jnp.logical_or(home != g, t != src))
            def _(src=src):
                part_landed(src).wait_recv()

    for way in range(2):

        @pl.when(sends(2, way, 1))
        def _(way=way):
            line(2, way, 1).start()

    for s in range(1, n_fs):
        for m in range(3):
            for way in range(2):

                @pl.when(gets(m, way, s))
                def _(m=m, way=way, s=s):
                    landed(m, way, s).wait_recv()
                    if s < n_fs - 1:

                        @pl.when(sends(m, way, s + 1))
                        def _():
                            line(m, way, s + 1).start()

                    if m < 2:
                        o = f - s if way == 0 else f + s
                        for dg in range(1, n_gr):
                            pair(m, dg, o).start()

    for m in range(2):
        for dg in range(1, n_gr):
            for o in range(n_fs):
                pair_landed(m, dg, o).wait_recv()
                pair(m, dg, o).wait_send()
    for m in range(3):
        for way in range(2):
            for s in range(1, n_fs):

                @pl.when(sends(m, way, s))
                def _(m=m, way=way, s=s):
                    line(m, way, s).wait_send()

    for dg in range(n_gr):
        if dg == 0:

            @pl.when(owner != t)
            def _():
                part(0).wait_send()

        else:
            part(dg).wait_send()


def gather(sizes, call, gain, gate, up, down):
    n_gr, n_fs, n_tp = sizes
    per = n_gr * n_fs // n_tp
    rows, width = gate.shape
    wide = rows % 128 == 0
    whole = (width, n_gr * n_fs * rows) if wide else (n_gr * n_fs, width, rows)
    tall, cols = down.shape
    vmem = pl.BlockSpec(memory_space=pltpu.VMEM)
    dma = pltpu.SemaphoreType.DMA
    gate_all, up_all, down_all = pl.pallas_call(
        functools.partial(gather_kernel, n_gr, n_fs, n_tp),
        out_shape=(
            jax.ShapeDtypeStruct(whole, jnp.bfloat16),
            jax.ShapeDtypeStruct(whole, jnp.bfloat16),
            jax.ShapeDtypeStruct((per, tall, n_tp * cols), jnp.bfloat16),
        ),
        in_specs=[vmem] * 4,
        out_specs=(vmem,) * 3,
        scratch_shapes=[
            pltpu.VMEM((tall, cols), jnp.bfloat16),
            dma((3, 2, n_fs)),
            dma((3, 2, n_fs)),
            dma((2, n_gr, n_fs)),
            dma((2, n_gr, n_fs)),
            dma((n_gr,)),
            dma((n_tp,)),
        ],
        compiler_params=pltpu.CompilerParams(
            collective_id=call, has_side_effects=True, vmem_limit_bytes=32 * 2**20
        ),
        cost_estimate=pl.CostEstimate(
            flops=10**10, bytes_accessed=16 * 2**20, transcendentals=0
        ),
    )(gain[None, :], gate.T, up.T, down)

    def upright(a):
        return a.T if wide else a.transpose(0, 2, 1).reshape(n_gr * n_fs * rows, width)

    return (
        upright(gate_all),
        upright(up_all),
        down_all.reshape(per * tall, n_tp * cols),
    )


SPLIT = ((3,), (3, 2))
SHARED = ((3, 7), (4, 2))
GROUPS = ((((0,), ()), ((1,), (0,))), (((0,), ()), ((), (0,)), ((1,), (1,))))


def laid(start, sizes):
    return tuple((start + sum(sizes[:i]), size) for i, size in enumerate(sizes))


def down_pieces(n, depth, column):
    unit = depth // 16
    split = [unit * size for size in SPLIT[n]]
    shared = [unit * size for size in SHARED[n]]
    return laid(sum(shared) + column * sum(split), split), laid(0, shared)


def column_ranges(n, depth, g):
    own, shared = down_pieces(n, depth, g)
    other, _ = down_pieces(n, depth, 1 - g)
    ranges = [((own[0][0], sum(size for _, size in own)),)]
    for whole, pieces in GROUPS[n]:
        ranges.append(tuple(shared[i] for i in whole) + tuple(other[i] for i in pieces))
    return ranges


INSIDE = 2


def fused_kernel(
    n_gr,
    n_fs,
    n_tp,
    prompt_in,
    gain_in_a,
    gate_in_a,
    up_in_a,
    down_in_a,
    gain_in_b,
    gate_in_b,
    up_in_b,
    down_in_b,
    gate_out_a,
    up_out_a,
    down_out_a,
    gate_out_b,
    up_out_b,
    down_out_b,
    mixed_ref,
    late_sums,
    late_rest,
    prompt,
    gains,
    tall_in,
    gates_in,
    load_sem,
    down_own,
    normed,
    normed_all,
    hidden,
    mate_out,
    mate_in,
    sums,
    sums_in,
    kept,
    stream,
    line_send,
    line_recv,
    pair_send,
    pair_recv,
    part_send,
    part_recv,
    mate_send,
    mate_recv,
    sum_send,
    sum_recv,
    row_send,
    row_recv,
):
    g, f, t = lax.axis_index("gr"), lax.axis_index("fs"), lax.axis_index("tp")
    per = n_gr * n_fs // n_tp
    tall, cols = down_in_a.shape
    width = gate_in_a.shape[1]
    owned, depth = prompt.shape[1], prompt.shape[2]
    first = lax.rem(t * per, n_fs)
    home = (t * per) // n_fs
    row = g * n_fs + f
    owner = row // per
    slot = lax.rem(row, per)
    pairs = n_tp // 2
    seat, core = t // 2, lax.rem(t, 2)
    outs = ((gate_out_a, up_out_a, down_out_a), (gate_out_b, up_out_b, down_out_b))

    carried = [2 + len(split) for split in SPLIT]
    count = [c + len(shared) for c, shared in zip(carried, SHARED)]

    def lanes(at, size):
        return pl.ds(pl.multiple_of(at, 128), size)

    barrier = pltpu.get_barrier_semaphore()
    for dg in range(n_gr):
        for dt in range(n_tp):
            if dg or dt:
                pl.semaphore_signal(
                    barrier,
                    inc=1,
                    device_id=(lax.rem(g + dg, n_gr), f, lax.rem(t + dt, n_tp)),
                    device_id_type=MESH,
                )
    for near, there in ((f + 1, f < n_fs - 1), (f - 1, f > 0)):

        @pl.when(there)
        def _(near=near):
            pl.semaphore_signal(barrier, inc=1, device_id=(g, near, t), device_id_type=MESH)

    between = jnp.logical_and(f > 0, f < n_fs - 1)
    greeted = n_gr * n_tp + jnp.where(between, 1, 0)

    loads = []
    for k, (src, dst) in enumerate(
        (
            (gain_in_a, gains.at[0]),
            (gate_in_a, gates_in.at[0]),
            (up_in_a, gates_in.at[1]),
            (down_in_a, tall_in.at[0]),
            (prompt_in, prompt),
            (gain_in_b, gains.at[1]),
            (down_in_b, tall_in.at[1]),
            (gate_in_b, gates_in.at[2]),
            (up_in_b, gates_in.at[3]),
        )
    ):
        load = pltpu.make_async_copy(src, dst, load_sem.at[k])
        load.start()
        loads.append(load)

    def place(ref, origin):
        return ref.at[:, pl.ds(pl.multiple_of(origin * width, 128), width)]

    def round_matrix(n, m):
        place(outs[n][m], row)[...] = (gains[n] * gates_in[2 * n + m]).astype(jnp.bfloat16)

    def round_down(n):
        rounded = tall_in[n].astype(jnp.bfloat16)
        down_own[n] = rounded

        @pl.when(owner == t)
        def _():
            outs[n][2][slot, :, lanes(t * cols, cols)] = rounded

    def held(o):
        return jnp.logical_and(o >= first, o < first + per)

    def remote(src, dst, send, recv, to):
        return pltpu.make_async_remote_copy(
            src_ref=src,
            dst_ref=dst,
            send_sem=send,
            recv_sem=recv,
            device_id=to,
            device_id_type=MESH,
        )

    def spot(n, p, o, column):
        if p < 2:
            return place(outs[n][p], column * n_fs + o)
        split, shared = down_pieces(n, depth, column)
        at, size = (split + shared)[p - 2]
        return outs[n][2].at[o - first, :, lanes(at, size)]

    def down_index(n, p):
        return n * (count[0] - 2) + p - 2

    def send_seat(n, p, o):
        if p < 2:
            return 2 * n + p
        return 4 + down_index(n, p) * (per + 1) + o - first

    def recv_seat(n, p, o):
        if p < 2:
            return (2 * n + p) * n_fs + o
        return 4 * n_fs + down_index(n, p) * per + o - first

    def line_sems(n, p, way, s, o):
        own = per + first if s == 1 and way == 1 else o
        return line_send.at[send_seat(n, p, own)], line_recv.at[recv_seat(n, p, o)]

    def line(n, p, way, s):
        step = 1 if way == 0 else -1
        o = f - step * (s - 1)
        sems = line_sems(n, p, way, s, o)
        return remote(spot(n, p, o, g), spot(n, p, o, g), *sems, (g, f + step, t))

    def sends(p, way, s):
        step = 1 if way == 0 else -1
        o = f - step * (s - 1)
        fine = (f < n_fs - 1, o >= 0) if way == 0 else (f > 0, o <= n_fs - 1)
        ok = jnp.logical_and(*fine)
        return jnp.logical_and(ok, held(o)) if p >= 2 else ok

    def origin(way, s):
        return f - s if way == 0 else f + s

    def gets(p, way, s):
        o = origin(way, s)
        ok = o >= 0 if way == 0 else o <= n_fs - 1
        return jnp.logical_and(ok, held(o)) if p >= 2 else ok

    def ends(way):
        return f == n_fs - 1 if way == 0 else f == 0

    def landed(n, p, way, s):
        o = origin(way, s)
        sems = line_sems(n, p, 0, s, o)
        return remote(spot(n, p, o, g), spot(n, p, o, g), *sems, (g, f, t))

    def pair_seat(n, p, o):
        if p < 2:
            return 2 * n + p
        return 4 + (n * (carried[0] - 2) + p - 2) * per + o - first

    def pair(n, p, o):
        sems = pair_send.at[pair_seat(n, p, o)], pair_recv.at[pair_seat(n, p, o)]
        return remote(spot(n, p, o, g), spot(n, p, o, g), *sems, (1 - g, f, t))

    def pair_landed(n, p, o):
        sems = pair_send.at[pair_seat(n, p, o)], pair_recv.at[pair_seat(n, p, o)]
        return remote(spot(n, p, o, 1 - g), spot(n, p, o, 1 - g), *sems, (1 - g, f, t))

    def part(n, dg):
        return remote(
            down_own.at[n],
            outs[n][2].at[slot, :, lanes(t * cols, cols)],
            part_send.at[n, dg],
            part_recv.at[n, t],
            (lax.rem(g + dg, n_gr), f, owner),
        )

    def part_landed(n, src):
        return remote(
            down_own.at[n],
            outs[n][2].at[f - first, :, pl.ds(src * cols, cols)],
            part_send.at[n, 0],
            part_recv.at[n, src],
            (home, f, src),
        )

    def start_lines(n, p):
        for way in range(2):

            @pl.when(sends(p, way, 1))
            def _(way=way):
                line(n, p, way, 1).start()

    def give_part(n):
        @pl.when(owner != t)
        def _():
            part(n, 0).start()

    def parts_in(n):
        @pl.when(held(f))
        def _():
            for src in range(n_tp):

                @pl.when(jnp.logical_or(home != g, t != src))
                def _(src=src):
                    part_landed(n, src).wait_recv()

    def forward(n, p, s):
        crosses, relays = p < carried[n], s < n_fs - 1
        for way in range(2):
            if not crosses and not relays:
                continue
            ready = gets(p, way, s)
            if not crosses:
                ready = jnp.logical_and(ready, jnp.logical_not(ends(way)))

            @pl.when(ready)
            def _(way=way):
                landed(n, p, way, s).wait_recv()
                if relays:

                    @pl.when(sends(p, way, s + 1))
                    def _():
                        line(n, p, way, s + 1).start()

                if crosses:
                    pair(n, p, origin(way, s)).start()

    def settle(n, p):
        for s in range(1, n_fs):
            for way in range(2):
                ready = gets(p, way, s)
                if s < n_fs - 1:
                    ready = jnp.logical_and(ready, ends(way))

                @pl.when(ready)
                def _(way=way, s=s):
                    landed(n, p, way, s).wait_recv()

    def blocks(n, p, origin, many, send, recv):
        at = pl.ds(pl.multiple_of(origin * width, 128), many * width)
        spot = outs[n][p].at[:, at]
        return remote(spot, spot, send, recv, (1 - g, f, t))

    def pair_blocks(n, p, column):
        sems = pair_send.at[pair_seat(n, p, 0)], pair_recv.at[pair_seat(n, p, 0)]
        return blocks(n, p, column * n_fs, n_fs, *sems)

    def pairs_in(n, p):
        if p < 2:
            pair_blocks(n, p, 1 - g).wait_recv()
            return
        for o in range(n_fs):

            @pl.when(jnp.logical_and(held(o), o != f))
            def _(o=o):
                pair_landed(n, p, o).wait_recv()

    def drain(n):
        for p in range(2):
            pair_blocks(n, p, g).wait_send()
            sems = line_send.at[send_seat(n, p, 0)], line_recv.at[recv_seat(n, p, 0)]

            @pl.when(between)
            def _(p=p, sems=sems):
                blocks(n, p, 0, n_fs + 1, *sems).wait_send()

            @pl.when(jnp.logical_not(between))
            def _(p=p, sems=sems):
                blocks(n, p, 0, 1, *sems).wait_send()

        for p in range(2, carried[n]):
            for o in range(n_fs):

                @pl.when(jnp.logical_and(held(o), o != f))
                def _(p=p, o=o):
                    pair(n, p, o).wait_send()

        for p in range(2, count[n]):
            for way in range(2):
                for s in range(1, n_fs):

                    @pl.when(sends(p, way, s))
                    def _(p=p, way=way, s=s):
                        line(n, p, way, s).wait_send()

        @pl.when(owner != t)
        def _():
            part(n, 0).wait_send()

        part(n, 1).wait_send()

    across = (((1,), (1,)), ((), ()))

    def unit(rows):
        return rows * lax.rsqrt(jnp.mean(rows * rows, axis=-1, keepdims=True) + 1e-06)

    def seat_of(j):
        return lax.rem(seat + 1 + j, pairs)

    def hide(n, source):
        @pl.loop(0, 2)
        def _(c):
            rows = jnp.concatenate([source[c, seat_of(j)] for j in range(pairs)], axis=0)
            gate = lax.dot_general(
                rows, outs[n][0][...], across, preferred_element_type=jnp.float32
            )
            upper = lax.dot_general(
                rows, outs[n][1][...], across, preferred_element_type=jnp.float32
            )
            hidden[c] = (jax.nn.silu(gate) * upper).astype(jnp.bfloat16)

    ranges = [column_ranges(n, depth, g) for n in range(2)]
    steps = [len(part) for part in ranges]
    widths = [[sum(size for _, size in columns) for columns in part] for part in ranges]
    starts = [[sum(sizes[:k]) for k in range(len(sizes))] for sizes in widths]
    spans = [[pl.ds(*at) for at in zip(starts[n], widths[n])] for n in range(2)]
    kernel_groups = (range(steps[0]), range(INSIDE))

    def mate(n, k):
        at = spans[n][k]
        return remote(
            mate_out.at[n, :, at],
            mate_in.at[n, :, at],
            mate_send.at[n],
            mate_recv.at[n, k],
            (g, f, t + 1 - 2 * core),
        )

    def share(n, k, j):
        at = spans[n][k]
        return remote(
            sums.at[n, j, :, at],
            sums_in.at[n, j, :, at],
            sum_send.at[n, j],
            sum_recv.at[n, k, j],
            (g, f, 2 * seat_of(j) + core),
        )

    def term(n, units, k):
        tiles = [
            jnp.dot(
                units,
                outs[n][2][:, :, lanes(at, size)].reshape(per * tall, size),
                preferred_element_type=jnp.float32,
            )
            for at, size in ranges[n][k]
        ]
        return tiles[0] if len(tiles) == 1 else jnp.concatenate(tiles, axis=1)

    def arrive(n, k):
        whole, pieces = GROUPS[n][k - 1]
        for i in whole:
            settle(n, carried[n] + i)
        for i in pieces:
            pairs_in(n, 2 + i)

    def offer(n, k):
        mate_out[n, :, spans[n][k]] = term(n, hidden[1 - core], k).astype(jnp.bfloat16)
        mate(n, k).start()

    def reduce(n, k):
        at = spans[n][k]
        mine = term(n, hidden[core], k)
        mate(n, k).wait_recv()
        both = mine + mate_in[n, :, at].astype(jnp.float32)
        if k in kernel_groups[n]:
            for j in range(pairs - 1):
                sums[n, j, :, at] = both[j * owned : (j + 1) * owned].astype(jnp.bfloat16)
                share(n, k, j).start()
            kept[:, at] = both[(pairs - 1) * owned :]
            return
        late = starts[n][k] - starts[n][INSIDE]
        for j in range(pairs - 1):
            late_sums[j, :, pl.ds(late, widths[n][k])] = both[j * owned : (j + 1) * owned].astype(
                jnp.bfloat16
            )
        passed = (pairs - 1) * owned
        done = 0
        for column, size in ranges[n][k]:
            late_rest[:, pl.ds(late + done, size)] = (
                stream[:, lanes(column, size)] + 0.5 * both[passed:, done : done + size]
            )
            done += size

    def collect(n, k, base, finish):
        for j in range(pairs - 1):
            share(n, k, j).wait_recv()
        total = kept[:, spans[n][k]]
        for j in range(pairs - 1):
            total += sums_in[n, j, :, spans[n][k]].astype(jnp.float32)
        passed = 0
        for at, size in ranges[n][k]:
            finish(lanes(at, size), base(lanes(at, size)) + 0.5 * total[:, passed : passed + size])
            passed += size

    def give(j):
        own = normed_all.at[core, seat]
        return remote(own, own, row_send.at[j], row_recv.at[j], (g, f, 2 * seat_of(j) + core))

    def given(j):
        src = lax.rem(seat - 1 - j + pairs, pairs)
        spot = normed_all.at[core, src]
        return remote(spot, spot, row_send.at[j], row_recv.at[j], (g, f, 2 * src + core))

    def pass_on(j):
        src = lax.rem(seat - 1 - j + 2 * pairs, pairs)
        spot = normed_all.at[core, src]
        at = pairs - 1 + (pairs - 1 if j < 0 else j)
        return remote(
            spot, spot, row_send.at[at], row_recv.at[at], (g, f, t + 1 - 2 * core)
        )

    def passed_on(j):
        src = lax.rem(seat - 1 - j + 2 * pairs, pairs)
        spot = normed_all.at[1 - core, src]
        at = pairs - 1 + (pairs - 1 if j < 0 else j)
        return remote(
            spot, spot, row_send.at[at], row_recv.at[at], (g, f, t + 1 - 2 * core)
        )

    loads[0].wait()
    loads[1].wait()
    round_matrix(0, 0)
    pl.semaphore_wait(barrier, greeted)
    start_lines(0, 0)
    pair(0, 0, f).start()
    loads[2].wait()
    round_matrix(0, 1)
    start_lines(0, 1)
    pair(0, 1, f).start()
    loads[3].wait()
    round_down(0)
    part(0, 1).start()
    give_part(0)
    loads[5].wait()
    loads[6].wait()
    round_down(1)
    give_part(1)
    loads[7].wait()
    round_matrix(1, 0)
    loads[8].wait()
    round_matrix(1, 1)
    loads[4].wait()

    @pl.loop(0, n_tp)
    def _(i):
        normed[lax.rem(i, 2), i // 2] = unit(prompt[i].astype(jnp.float32)).astype(jnp.bfloat16)

    def forward_both(n, s):
        for m in range(2):
            forward(n, m, s)

    def forward_piece(n, p):
        for s in range(1, n_fs):
            forward(n, p, s)

    def spread(n, ks):
        for i, k in enumerate(ks):
            if k:
                arrive(n, k)
            offer(n, k)
            if i:
                reduce(n, ks[i - 1])
        reduce(n, ks[-1])

    middle = n_fs // 2
    for s in range(1, middle + 1):
        forward_both(0, s)
    parts_in(0)
    for p in range(2, carried[0] + 1):
        start_lines(0, p)
    for s in range(middle + 1, n_fs):
        forward_both(0, s)
    for p in range(2, carried[0] + 1):
        forward_piece(0, p)
    part(1, 1).start()
    for m in range(2):
        start_lines(1, m)
        pair(1, m, f).start()
    for p in range(carried[0] + 1, count[0]):
        start_lines(0, p)
    for p in range(carried[0] + 1, count[0]):
        forward_piece(0, p)
    for m in range(2):
        pairs_in(0, m)
    hide(0, normed)
    spread(0, range(steps[0] - 1))
    forward_both(1, 1)
    spread(0, [steps[0] - 1])
    for s in range(2, middle + 1):
        forward_both(1, s)

    def own_prompt(at):
        return prompt[t, :, at].astype(jnp.float32)

    def keep_stream(at, value):
        stream[:, at] = value

    for k in range(steps[0]):
        collect(0, k, own_prompt, keep_stream)
    normed_all[core, seat] = unit(stream[...]).astype(jnp.bfloat16)
    for j in range(pairs - 1):
        give(j).start()
    pass_on(-1).start()
    parts_in(1)
    for p in range(2, count[1]):
        start_lines(1, p)
    for s in range(middle + 1, n_fs):
        forward_both(1, s)
    for j in range(pairs - 1):
        given(j).wait_recv()
        pass_on(j).start()
    for p in range(2, count[1]):
        forward_piece(1, p)
    drain(0)
    for j in range(-1, pairs - 1):
        passed_on(j).wait_recv()
    for m in range(2):
        pairs_in(1, m)
    hide(1, normed_all)

    def keep_mixed(at, value):
        mixed_ref[:, at] = value.astype(jnp.bfloat16)

    def own_stream(at):
        return stream[:, at]

    for k in range(steps[1]):
        spread(1, [k])
    drain(1)
    for k in kernel_groups[1]:
        collect(1, k, own_stream, keep_mixed)
    for j in range(pairs - 1):
        give(j).wait_send()
    for j in range(-1, pairs - 1):
        pass_on(j).wait_send()
    for n in range(2):
        spot = mate_out.at[n]
        remote(
            spot, spot, mate_send.at[n], mate_recv.at[n, 0], (g, f, t + 1 - 2 * core)
        ).wait_send()
        whole = pl.ds(0, sum(widths[n][k] for k in kernel_groups[n]))
        for j in range(pairs - 1):
            spot = sums.at[n, j, :, whole]
            remote(
                spot, spot, sum_send.at[n, j], sum_recv.at[n, 0, j], (g, f, 2 * seat_of(j) + core)
            ).wait_send()


def write_kernel(*refs):
    count = (len(refs) - 1) // 2
    sems = refs[-1]
    copies = [
        pltpu.make_async_copy(refs[k], refs[count + k], sems.at[k]) for k in range(count)
    ]
    for copy in copies:
        copy.start()
    for copy in copies:
        copy.wait()


def written(arrays):
    arrays = [pltpu.with_memory_space_constraint(a, pltpu.VMEM) for a in arrays]
    return pl.pallas_call(
        write_kernel,
        out_shape=tuple(jax.ShapeDtypeStruct(a.shape, a.dtype) for a in arrays),
        in_specs=[pl.BlockSpec(memory_space=pltpu.VMEM)] * len(arrays),
        out_specs=(pl.BlockSpec(memory_space=pl.ANY),) * len(arrays),
        scratch_shapes=[pltpu.SemaphoreType.DMA((len(arrays),))],
        compiler_params=pltpu.CompilerParams(vmem_limit_bytes=2**20),
        cost_estimate=pl.CostEstimate(
            flops=2 * 10**9, bytes_accessed=32 * 2**20, transcendentals=0
        ),
    )(*arrays)


def finish_kernel(early_ref, rest_ref, *refs):
    mixed_ref = refs[-1]
    depth = early_ref.shape[1]
    total = rest_ref[...]
    for received in refs[:-1]:
        total += 0.5 * received[...].astype(jnp.float32)
    total = total.astype(mixed_ref.dtype)
    ranges = column_ranges(1, depth, lax.axis_index("gr"))
    done = 0
    for k, columns in enumerate(ranges):
        for at, size in columns:
            at = pl.ds(pl.multiple_of(at, 128), size)
            if k < INSIDE:
                mixed_ref[:, at] = early_ref[:, at]
            else:
                mixed_ref[:, at] = total[:, done : done + size]
                done += size


def finished(early, rest, received):
    return pl.pallas_call(
        finish_kernel,
        out_shape=jax.ShapeDtypeStruct(early.shape, early.dtype),
        compiler_params=pltpu.CompilerParams(vmem_limit_bytes=4 * 2**20),
    )(early, rest, *received)


def fused(sizes, prompt, *weights):
    n_gr, n_fs, n_tp = sizes
    per = n_gr * n_fs // n_tp
    tokens, depth = prompt.shape
    owned = tokens // n_tp
    rows, width = weights[1].shape
    tall, cols = weights[3].shape
    pairs = n_tp // 2
    steps = 1 + max(len(groups) for groups in GROUPS)
    crossing, pieces = sum(map(len, SPLIT)), sum(map(len, SPLIT + SHARED))
    late = sum(size for columns in column_ranges(1, depth, 0)[INSIDE:] for _, size in columns)
    vmem = pl.BlockSpec(memory_space=pltpu.VMEM)
    hbm = pl.BlockSpec(memory_space=pltpu.HBM)
    dma = pltpu.SemaphoreType.DMA
    across = pltpu.VMEM((width, n_gr * n_fs * rows), jnp.bfloat16)
    down = pltpu.VMEM((per, tall, n_tp * cols), jnp.bfloat16)
    operands = [prompt.reshape(n_tp, owned, depth)]
    for n in range(2):
        gain, gate, up, tall_block = weights[4 * n : 4 * n + 4]
        operands += [gain[None, :], gate.T, up.T, tall_block]
    results = pl.pallas_call(
        functools.partial(fused_kernel, n_gr, n_fs, n_tp),
        out_shape=(across, across, down) * 2
        + (
            pltpu.VMEM((owned, depth), jnp.bfloat16),
            pltpu.VMEM((pairs - 1, owned, late), jnp.bfloat16),
            pltpu.VMEM((owned, late), jnp.float32),
        ),
        in_specs=[hbm] * 9,
        out_specs=(vmem,) * 9,
        scratch_shapes=[
            pltpu.VMEM((n_tp, owned, depth), prompt.dtype),
            pltpu.VMEM((2, 1, rows), jnp.float32),
            pltpu.VMEM((2, tall, cols), jnp.float32),
            pltpu.VMEM((4, width, rows), jnp.float32),
            dma((9,)),
            pltpu.VMEM((2, tall, cols), jnp.bfloat16),
            pltpu.VMEM((2, pairs, owned, depth), jnp.bfloat16),
            pltpu.VMEM((2, pairs, owned, depth), jnp.bfloat16),
            pltpu.VMEM((2, pairs * owned, width), jnp.bfloat16),
            pltpu.VMEM((2, pairs * owned, depth), jnp.bfloat16),
            pltpu.VMEM((2, pairs * owned, depth), jnp.bfloat16),
            pltpu.VMEM((2, pairs - 1, owned, depth), jnp.bfloat16),
            pltpu.VMEM((2, pairs - 1, owned, depth), jnp.bfloat16),
            pltpu.VMEM((owned, depth), jnp.float32),
            pltpu.VMEM((owned, depth), jnp.float32),
            dma((4 + pieces * (per + 1),)),
            dma((4 * n_fs + pieces * per,)),
            dma((4 + crossing * per,)),
            dma((4 + crossing * per,)),
            dma((2, n_gr)),
            dma((2, n_tp)),
            dma((2,)),
            dma((2, steps)),
            dma((2, pairs - 1)),
            dma((2, steps, pairs - 1)),
            dma((2 * pairs - 1,)),
            dma((2 * pairs - 1,)),
        ],
        compiler_params=pltpu.CompilerParams(
            collective_id=2, has_side_effects=True, vmem_limit_bytes=44 * 2**20
        ),
    )(*operands)
    *served, early, sums, rest = results
    received = [
        lax.ppermute(
            sums[j], "tp", [(t, (t + 2 * (1 + j)) % n_tp) for t in range(n_tp)]
        )
        for j in range(pairs - 1)
    ]
    gate_a, up_a, down_a, gate_b, up_b, down_b = written(served)
    mixed = finished(early, rest, received)

    def flat(a):
        return a.reshape(per * tall, n_tp * cols)

    return (gate_a.T, up_a.T, flat(down_a), gate_b.T, up_b.T, flat(down_b), mixed)


def normalize(rows):
    rows = rows.astype(jnp.float32)
    scale = lax.rsqrt(jnp.mean(rows * rows, axis=-1, keepdims=True) + 1e-06)
    return (rows * scale).astype(jnp.bfloat16)


def hidden_units(normed, w_gate, w_up):
    gate = jnp.dot(normed, w_gate, preferred_element_type=jnp.float32)
    upper = jnp.dot(normed, w_up, preferred_element_type=jnp.float32)
    return (jax.nn.silu(gate) * upper).astype(jnp.bfloat16)


def rounded_term(hidden, w_down):
    return jnp.dot(hidden, w_down, preferred_element_type=jnp.float32).astype(jnp.bfloat16)


def suits(sizes, prompt, gate, down):
    n_gr, n_fs, n_tp = sizes
    per = n_gr * n_fs // n_tp
    return (
        n_gr == 2
        and n_tp % 2 == 0
        and per > 0
        and per * n_tp == n_gr * n_fs
        and n_fs % per == 0
        and gate.shape[0] % 128 == 0
        and down.shape[0] % 16 == 0
        and down.shape[1] % 128 == 0
        and prompt.shape[1] % 2048 == 0
        and prompt.shape[0] % (16 * n_tp) == 0
    )


def shards(
    sizes,
    prompt,
    gain_first,
    gate_first,
    up_first,
    down_first,
    gain_second,
    gate_second,
    up_second,
    down_second,
):
    if suits(sizes, prompt, gate_first, down_first):
        return fused(
            sizes,
            prompt,
            gain_first,
            gate_first,
            up_first,
            down_first,
            gain_second,
            gate_second,
            up_second,
            down_second,
        )
    gate_a, up_a, down_a = gather(sizes, 0, gain_first, gate_first, up_first, down_first)
    hidden_a = hidden_units(normalize(prompt), gate_a, up_a)
    term_a = rounded_term(hidden_a, down_a)
    term_a, gain_second = lax.optimization_barrier((term_a, gain_second))
    branch_a = lax.psum(term_a, "tp").astype(jnp.float32)
    gate_b, up_b, down_b = gather(sizes, 1, gain_second, gate_second, up_second, down_second)
    stream = prompt.astype(jnp.float32) + 0.5 * branch_a
    hidden_b = hidden_units(normalize(stream), gate_b, up_b)
    owned = hidden_b.shape[0] // lax.axis_size("tp")
    branch_b = lax.psum_scatter(
        rounded_term(hidden_b, down_b), "tp", scatter_dimension=0, tiled=True
    ).astype(jnp.float32)
    own_stream = lax.dynamic_slice_in_dim(stream, lax.axis_index("tp") * owned, owned, 0)
    mixed = (own_stream + 0.5 * branch_b).astype(jnp.bfloat16)
    return (gate_a, up_a, down_a, gate_b, up_b, down_b, mixed)


def solution(mesh):
    sizes = (mesh.shape["gr"], mesh.shape["fs"], mesh.shape["tp"])
    return jax.shard_map(
        functools.partial(shards, sizes),
        mesh=mesh,
        in_specs=(
            P(("gr", "fs"), None),
            P(("gr", "fs")),
            P(("gr", "fs"), "tp"),
            P(("gr", "fs"), "tp"),
            P(("gr", "fs"), "tp"),
            P(("gr", "fs")),
            P(("gr", "fs"), "tp"),
            P(("gr", "fs"), "tp"),
            P(("gr", "fs"), "tp"),
        ),
        out_specs=(
            P(None, "tp"),
            P(None, "tp"),
            P("tp", None),
            P(None, "tp"),
            P(None, "tp"),
            P("tp", None),
            P(("gr", "fs", "tp"), None),
        ),
        check_vma=False,
    )
```
